32 devices in a mesh: ep: 4 (over y, x), tp: 8 (over z, core).
Axes of the slice: x: 2, y: 2, z: 4, core: 2. Of those that a mesh axis runs over, the one named last changes fastest.
Arguments:
- residual: bfloat16 [128, 2048], P('ep'), may hold values from -20 to 20
- cache_latent: bfloat16 [128, 2048, 256], P(('ep', 'tp')), may hold values from -12 to 12
- cache_rope: bfloat16 [128, 32, 2048], P(('ep', 'tp')), may hold values from -6 to 6
- lengths: int32 [128], P(('ep', 'tp')), may hold values from 2 to 2048, as said below
- query_latent: bfloat16 [128, 32, 256], P(('ep', 'tp')), may hold values from -250 to 250
- query_rope: bfloat16 [128, 32, 32], P(('ep', 'tp')), may hold values from -6 to 6
- norm_gain: bfloat16 [2048], replicated, may hold values from 0.099609375 to 1.8984375
- latent_weight: bfloat16 [2048, 256], replicated, may hold values from -0.125 to 0.125
- latent_gain: bfloat16 [256], replicated, may hold values from 0.099609375 to 1.8984375
- rope_weight: bfloat16 [32, 2048], replicated, may hold values from -0.125 to 0.125
- value_weight: bfloat16 [256, 2048], replicated, may hold values from -0.375 to 0.375
- out_weight: bfloat16 [2048, 2048], P('tp'), may hold values from -1 to 1
- mixer_gain: bfloat16 [2048], replicated, may hold values from 0.099609375 to 1.8984375
- group_router: bfloat16 [2048, 4], replicated, may hold values from -0.0625 to 0.0625
- expert_router: bfloat16 [2048, 8], replicated, may hold values from -0.0625 to 0.0625
- expert_ids: int32 [128, 2], P('ep'), may hold values from 0 to 7, as said below
- gate_weight: bfloat16 [8, 2048, 4096], P('ep', None, 'tp'), may hold values from -0.125 to 0.125
- up_weight: bfloat16 [8, 2048, 4096], P('ep', None, 'tp'), may hold values from -0.125 to 0.125
- down_weight: bfloat16 [8, 4096, 2048], P('ep', 'tp'), may hold values from -0.75 to 0.75
Outputs:
- mixed: bfloat16 [128, 2048], P('ep')
- new_latent: bfloat16 [128, 256], P(('ep', 'tp'))
- new_rope_key: bfloat16 [128, 32], P(('ep', 'tp'))
The draws below stay inside these ranges and needn't reach their ends.
Inputs may be any that keep to these rules, and one draw needn't show every extreme that they name: `lengths`: every sequence has 2 or more cached positions, and in every draw some sequence has all 2048. `expert_ids`: each row names 2 different experts of one group; group g holds experts g * 2 to g * 2 + 1. Among the rows of one index of ep (aligned blocks of 32 rows) no expert is named more than 16 times, and in every draw some expert is named exactly 16 times in every block.
All inputs are finite; a program needn't handle non-finite values.
Results may differ from the reference program's by a relative error of at most 0.012.
Values may be sent and summed in bfloat16 or wider, within the bound.
No kernel may reach another device: no remote copies, remote signals or barrier semaphores. Data moves between devices by JAX's collectives and lax.ppermute only.
A program may use at most 64 MiB of HBM per device.

```python
import math
from functools import partial
import jax
import jax.numpy as jnp
from jax import lax

D = 2048
H = 32
KV = 256
ROPE = 32
NOPE = 64
V = 64
DE = 4096
GROUPS = 4
TOPK = 2
LEN = 2048
GROUP_SEQS = 32
SEQS = 128
EXPERTS = 8
CAP = 16
N_EP = 4


def anchor_rows(key):
    base_key = jax.random.fold_in(key, 7)
    first_rows = jax.random.normal(jax.random.fold_in(base_key, 1), (SEQS, KV), jnp.float32)
    other_rows = jax.random.normal(jax.random.fold_in(base_key, 2), (SEQS, KV), jnp.float32)
    return (first_rows, other_rows)


def draw_cache_latent(key, part):
    first_rows, other_rows = anchor_rows(key)
    remaining = jax.random.normal(jax.random.fold_in(key, 3), (SEQS, LEN - 2, KV), jnp.float32)
    whole = jnp.concatenate([first_rows[:, None, :], other_rows[:, None, :], remaining], axis=1)
    return jnp.clip(whole, -12.0, 12.0).astype(jnp.bfloat16)


def draw_query_latent(key, part):
    values = jax.random.normal(jax.random.fold_in(key, 5), (SEQS, H, KV), jnp.float32)
    return jnp.clip(values, -250.0, 250.0).astype(jnp.bfloat16)


def draw_residual(key, part):
    base_key = jax.random.fold_in(key, 13)
    column_scale = jnp.exp(jax.random.uniform(jax.random.fold_in(base_key, 1), (D,), jnp.float32, math.log(0.3), math.log(3.0)))
    values = jax.random.normal(jax.random.fold_in(base_key, 2), (SEQS, D), jnp.float32)
    return jnp.clip(values * column_scale[None, :], -20.0, 20.0).astype(jnp.bfloat16)


def draw_lengths(key, part):
    base_key = jax.random.fold_in(key, 17)
    exponent = jax.random.randint(jax.random.fold_in(base_key, 1), (SEQS,), 1, 14)
    spans = jnp.left_shift(jnp.ones((SEQS,), jnp.int32), exponent.astype(jnp.int32))
    drawn = 2 + jax.random.randint(jax.random.fold_in(base_key, 2), (SEQS,), 0, spans)
    drawn = jnp.minimum(drawn, LEN)
    chosen = jax.random.randint(jax.random.fold_in(base_key, 3), (), 0, SEQS)
    return jnp.where(jnp.arange(SEQS) == chosen, LEN, drawn).astype(jnp.int32)


def draw_expert_ids(key, part):
    base_key = jax.random.fold_in(key, 19)
    per_group = EXPERTS // GROUPS
    half_rows = GROUP_SEQS // 2
    busiest = jax.random.randint(jax.random.fold_in(base_key, 1), (), 0, GROUPS).astype(jnp.int32)

    def one_block(block_key):
        others = (busiest + jax.random.randint(jax.random.fold_in(block_key, 1), (GROUP_SEQS - half_rows,), 1, GROUPS)) % GROUPS
        chosen = jnp.concatenate([jnp.full((half_rows,), busiest, jnp.int32), others.astype(jnp.int32)])
        hit_table = (chosen[:, None] == jnp.arange(GROUPS, dtype=jnp.int32)[None, :]).astype(jnp.int32)
        order_in_group = jnp.sum((jnp.cumsum(hit_table, axis=0) - hit_table) * hit_table, axis=1)
        offsets = jax.random.randint(jax.random.fold_in(block_key, 2), (GROUPS,), 0, per_group)
        orders = jax.vmap(lambda sub_key: jax.random.permutation(sub_key, per_group))(jax.random.split(jax.random.fold_in(block_key, 3), GROUPS))
        first_slot = (offsets[chosen] + 2 * order_in_group) % per_group
        second_slot = (first_slot + 1) % per_group
        first_id = chosen * per_group + orders[chosen, first_slot]
        second_id = chosen * per_group + orders[chosen, second_slot]
        paired = jnp.stack([first_id, second_id], axis=1)
        shuffle = jax.random.permutation(jax.random.fold_in(block_key, 4), GROUP_SEQS)
        return paired[shuffle]
    block_keys = jax.random.split(jax.random.fold_in(base_key, 2), SEQS // GROUP_SEQS)
    return jax.vmap(one_block)(block_keys).reshape(SEQS, TOPK).astype(jnp.int32)


def spiked(values, stream_key, source, target, blocks, factor):
    owner, partner = [(jnp.arange(values.shape[dim]) // (values.shape[dim] // blocks)).reshape([-1 if axis == dim else 1 for axis in range(values.ndim)]) for dim in (source, target)]
    chosen = jax.random.permutation(stream_key, blocks)[partner]
    strong = (owner == chosen) | (owner == (partner + blocks // 2) % blocks)
    return jnp.where(strong, factor * values, values)


def block_scale(key, shape, pieces, low, largest):
    loudness, own = 1.0, jax.random.fold_in(key, 6)
    for dim, blocks in pieces:
        draws = jnp.exp(jax.random.uniform(jax.random.fold_in(own, dim), (blocks,), jnp.float32, low / len(pieces), largest / len(pieces)))
        loudness = loudness * jnp.repeat(draws, shape[dim] // blocks).reshape([-1 if axis == dim else 1 for axis in range(len(shape))])
    return loudness


def gaussian(key, extent, scale, reach, cuts=(), kind=jnp.bfloat16):
    values = jax.random.normal(key, extent, jnp.float32) * scale
    if len(cuts) > 0:
        values = block_scale(key, extent, cuts, -0.22, 0.18) * values
    return jnp.clip(values, min=-reach, max=reach).astype(kind)


def bell_draw_with(stream_key, dims, spread, limit, cuts, heavy, held_as=jnp.bfloat16):
    result = spread * jax.random.normal(stream_key, dims, jnp.float32)
    if cuts:
        result = result * block_scale(stream_key, dims, cuts, -0.22, 0.18)
    return jnp.clip(spiked(result, jax.random.fold_in(stream_key, 3), *heavy), -limit, limit).astype(held_as)


def setup_inputs(seed: int = 0) -> dict:
    splits = jax.random.split(jax.random.key(seed), 20)
    residual = draw_residual(jax.random.fold_in(splits[19], 71), 0)
    cache_latent = draw_cache_latent(jax.random.fold_in(splits[19], 71), 0)
    cache_rope = gaussian(splits[2], (SEQS, ROPE, LEN), 1.0, 6.0, ((0, 32),))
    lengths = draw_lengths(jax.random.fold_in(splits[19], 71), 0)
    query_latent = draw_query_latent(jax.random.fold_in(splits[19], 71), 0)
    query_rope = gaussian(splits[5], (SEQS, H, ROPE), 1.0, 6.0, ((0, 32),))
    norm_gain = jnp.clip(1.0 + 0.18 * jax.random.normal(splits[6], (D,), jnp.float32), 0.099609375, 1.8984375).astype(jnp.bfloat16)
    latent_weight = gaussian(splits[7], (D, KV), D ** -0.5, 0.125)
    latent_gain = jnp.clip(1.0 + 0.18 * jax.random.normal(splits[8], (KV,), jnp.float32), 0.099609375, 1.8984375).astype(jnp.bfloat16)
    rope_weight = gaussian(splits[9], (ROPE, D), D ** -0.5, 0.125)
    value_weight = gaussian(splits[10], (KV, H * V), KV ** -0.5, 0.375)
    out_weight = bell_draw_with(splits[11], (H * V, D), (H * V // 32) ** -0.5, 1.0, ((0, 8),), (0, 1, 8, 2.0))
    mixer_gain = jnp.clip(1.0 + 0.18 * jax.random.normal(splits[12], (D,), jnp.float32), 0.099609375, 1.8984375).astype(jnp.bfloat16)
    group_router = gaussian(splits[13], (D, GROUPS), (4 * D) ** -0.5, 0.0625)
    expert_router = gaussian(splits[14], (D, EXPERTS), (4 * D) ** -0.5, 0.0625)
    expert_ids = draw_expert_ids(jax.random.fold_in(splits[19], 71), 0)
    gate_weight = gaussian(splits[16], (EXPERTS, D, DE), D ** -0.5, 0.125, ((0, 4), (2, 8)))
    up_weight = gaussian(splits[17], (EXPERTS, D, DE), D ** -0.5, 0.125, ((0, 4), (2, 8)))
    down_weight = gaussian(splits[18], (EXPERTS, DE, D), (DE // 64) ** -0.5, 0.75, ((0, 4), (1, 8)))
    return {"residual": residual, "cache_latent": cache_latent, "cache_rope": cache_rope, "lengths": lengths, "query_latent": query_latent, "query_rope": query_rope, "norm_gain": norm_gain, "latent_weight": latent_weight, "latent_gain": latent_gain, "rope_weight": rope_weight, "value_weight": value_weight, "out_weight": out_weight, "mixer_gain": mixer_gain, "group_router": group_router, "expert_router": expert_router, "expert_ids": expert_ids, "gate_weight": gate_weight, "up_weight": up_weight, "down_weight": down_weight}


NORM_EPSILON = 1e-06
ROPE_BASE = 10000.0

def inverse_rms(values):
    return lax.rsqrt(lax.optimization_barrier(jnp.mean(values * values, axis=-1, keepdims=True)) + NORM_EPSILON)

def rotate(vector, position):
    half_width = vector.shape[-1] // 2
    frequency = ROPE_BASE ** (-jnp.arange(0, vector.shape[-1], 2, dtype=jnp.float32) / vector.shape[-1])
    angles = position[..., None] * frequency
    lower_half = vector[..., :half_width]
    upper_half = vector[..., half_width:]
    return jnp.concatenate([lower_half * jnp.cos(angles) - upper_half * jnp.sin(angles), upper_half * jnp.cos(angles) + lower_half * jnp.sin(angles)], axis=-1)

def dispatch_table(expert_rows, experts, capacity):
    flat_ids = expert_rows.reshape(-1)
    hit_table = (flat_ids[:, None] == jnp.arange(experts, dtype=jnp.int32)[None, :]).astype(jnp.int32)
    slot_rank = lax.optimization_barrier(jnp.sum((jnp.cumsum(hit_table, axis=0) - hit_table) * hit_table, axis=1))
    slot_index = flat_ids * capacity + slot_rank
    picked = (slot_index[None, :] == jnp.arange(experts * capacity, dtype=jnp.int32)[:, None]).astype(jnp.float32)
    return picked.reshape(experts * capacity, expert_rows.shape[0], expert_rows.shape[1])

def route_weights(expert_in, group_router, expert_router, expert_ids, per_group):
    group_logits = jnp.dot(expert_in, group_router, preferred_element_type=jnp.float32)
    expert_logits = jnp.dot(expert_in, expert_router, preferred_element_type=jnp.float32)
    chosen = expert_ids[:, 0] // per_group
    group_hit = (jnp.arange(group_logits.shape[1], dtype=jnp.int32)[None, :] == chosen[:, None]).astype(jnp.float32)
    chosen_logit = lax.optimization_barrier(jnp.sum(group_logits * group_hit, axis=1, keepdims=True))
    group_share = 1.0 / lax.optimization_barrier(jnp.sum(jnp.exp(group_logits - chosen_logit), axis=1))
    expert_hit = (expert_ids[:, :, None] == jnp.arange(expert_logits.shape[1], dtype=jnp.int32)[None, None, :]).astype(jnp.float32)
    picked_logit = lax.optimization_barrier(jnp.sum(expert_hit * expert_logits[:, None, :], axis=2))
    inner_share = 1.0 / lax.optimization_barrier(jnp.sum(jnp.exp(picked_logit[:, None, :] - picked_logit[:, :, None]), axis=2))
    return group_share[:, None] * inner_share

def attend_one(args):
    latent_rows, rope_rows, length, query_lat, query_rot, fresh_latent, fresh_rope = args
    score_scale = (NOPE + ROPE) ** (-0.5)
    cached = (jnp.dot(query_lat, latent_rows.T, preferred_element_type=jnp.float32) + jnp.dot(query_rot, rope_rows, preferred_element_type=jnp.float32)) * score_scale
    keeping = jnp.arange(latent_rows.shape[0], dtype=jnp.int32) < length
    cached = jnp.where(keeping[None, :], cached, -jnp.inf)
    fresh = (jnp.dot(query_lat, fresh_latent, preferred_element_type=jnp.float32) + jnp.dot(query_rot, fresh_rope, preferred_element_type=jnp.float32)) * score_scale
    row_top = jnp.maximum(lax.optimization_barrier(jnp.max(cached, axis=1)), fresh)
    cached_exp = jnp.exp(cached - row_top[:, None])
    fresh_exp = jnp.exp(fresh - row_top)
    denominator = lax.optimization_barrier(jnp.sum(cached_exp, axis=1)) + fresh_exp
    cached_weight = (cached_exp / denominator[:, None]).astype(jnp.bfloat16)
    fresh_weight = (fresh_exp / denominator).astype(jnp.bfloat16)
    combined = jnp.dot(cached_weight, latent_rows, preferred_element_type=jnp.float32) + fresh_weight.astype(jnp.float32)[:, None] * fresh_latent.astype(jnp.float32)[None, :]
    return combined.astype(jnp.bfloat16)

def run_expert(args):
    rows, gate_part, up_part, down_part = args
    gate_value = jnp.dot(rows, gate_part, preferred_element_type=jnp.float32)
    up_value = jnp.dot(rows, up_part, preferred_element_type=jnp.float32)
    activation = (jax.nn.silu(gate_value) * up_value).astype(jnp.bfloat16)
    return jnp.dot(activation, down_part, preferred_element_type=jnp.float32)

def reference(residual, cache_latent, cache_rope, lengths, query_latent, query_rope, norm_gain, latent_weight, latent_gain, rope_weight, value_weight, out_weight, mixer_gain, group_router, expert_router, expert_ids, gate_weight, up_weight, down_weight):
    resid_f = residual.astype(jnp.float32)
    normed = (resid_f * inverse_rms(resid_f) * norm_gain.astype(jnp.float32)).astype(jnp.bfloat16)
    latent_raw = jnp.dot(normed, latent_weight, preferred_element_type=jnp.float32)
    new_latent = (latent_raw * inverse_rms(latent_raw) * latent_gain.astype(jnp.float32)).astype(jnp.bfloat16)
    positions = lengths.astype(jnp.float32)
    rope_raw = jnp.dot(normed, rope_weight.T, preferred_element_type=jnp.float32)
    new_rope_key = rotate(rope_raw, positions).astype(jnp.bfloat16)
    query_turned = rotate(query_rope.astype(jnp.float32), positions[:, None]).astype(jnp.bfloat16)
    mixed_latent = lax.map(attend_one, (cache_latent, cache_rope, lengths, query_latent, query_turned, new_latent, new_rope_key))
    head_values = jnp.einsum('shc,chv->shv', mixed_latent.astype(jnp.float32), value_weight.reshape(KV, H, V).astype(jnp.float32)).astype(jnp.bfloat16)
    attended = jnp.dot(head_values.reshape(SEQS, H * V), out_weight, preferred_element_type=jnp.float32)
    after_attention = (resid_f + attended).astype(jnp.bfloat16)
    after_f = after_attention.astype(jnp.float32)
    expert_in = (after_f * inverse_rms(after_f) * mixer_gain.astype(jnp.float32)).astype(jnp.bfloat16)
    route_weight = route_weights(expert_in, group_router, expert_router, expert_ids, EXPERTS // GROUPS)
    ids_blocks = expert_ids.reshape(N_EP, GROUP_SEQS, TOPK)
    picked = jax.vmap(partial(dispatch_table, experts=EXPERTS, capacity=CAP))(ids_blocks)
    select_rows = lax.optimization_barrier(jnp.sum(picked, axis=3))
    outbound = jnp.einsum('bsr,brd->bsd', select_rows, expert_in.reshape(N_EP, GROUP_SEQS, D).astype(jnp.float32), precision=lax.Precision.HIGHEST).astype(jnp.bfloat16)
    per_expert = outbound.reshape(N_EP, EXPERTS, CAP, D).transpose(1, 0, 2, 3).reshape(EXPERTS, N_EP * CAP, D)
    expert_out = lax.map(run_expert, (per_expert, gate_weight, up_weight, down_weight))
    back_blocks = expert_out.reshape(EXPERTS, N_EP, CAP, D).transpose(1, 0, 2, 3).reshape(N_EP, EXPERTS * CAP, D)
    combine = lax.optimization_barrier(jnp.sum(picked * route_weight.reshape(N_EP, 1, GROUP_SEQS, TOPK), axis=3))
    moe_sum = jnp.einsum('bsr,bsd->brd', combine, back_blocks, precision=lax.Precision.HIGHEST).reshape(SEQS, D)
    mixed = (after_f + moe_sum).astype(jnp.bfloat16)
    return (mixed, new_latent, new_rope_key)
```

```python
import jax
import jax.numpy as jnp
from jax import lax
from jax.sharding import PartitionSpec as P

H = 32
KV = 256
ROPE = 32
NOPE = 64
V = 64
GROUPS = 4
TOPK = 2


NORM_EPSILON = 1e-06
ROPE_BASE = 10000.0


def inverse_rms(values):
    return lax.rsqrt(jnp.mean(values * values, axis=-1, keepdims=True) + NORM_EPSILON)


def rotate(vector, position):
    half_width = vector.shape[-1] // 2
    frequency = ROPE_BASE ** (
        -jnp.arange(0, vector.shape[-1], 2, dtype=jnp.float32) / vector.shape[-1]
    )
    angles = position[..., None] * frequency
    lower_half = vector[..., :half_width]
    upper_half = vector[..., half_width:]
    return jnp.concatenate(
        [
            lower_half * jnp.cos(angles) - upper_half * jnp.sin(angles),
            upper_half * jnp.cos(angles) + lower_half * jnp.sin(angles),
        ],
        axis=-1,
    )


def slot_table(expert_ids, ep_count, local_experts, slots):
    hits = jnp.any(
        (expert_ids // local_experts)[:, :, None]
        == jnp.arange(ep_count, dtype=jnp.int32)[None, None, :],
        axis=1,
    )
    row = jnp.arange(expert_ids.shape[0], dtype=jnp.int32)
    earlier = (row[None, :] < row[:, None]).astype(jnp.float32)
    rank = jnp.dot(earlier, hits.astype(jnp.float32))
    slot = jnp.arange(slots, dtype=jnp.float32)
    picked = (rank.T[:, None, :] == slot[None, :, None]) & hits.T[:, None, :]
    return picked.astype(jnp.float32)


def gather_copies(block, axis):
    copies = jnp.broadcast_to(block[None], (lax.axis_size(axis),) + block.shape)
    return lax.all_to_all(copies, axis, split_axis=0, concat_axis=0, tiled=True)


def route_weights(expert_in, group_router, expert_router, expert_ids, per_group):
    group_logits = jnp.dot(expert_in, group_router, preferred_element_type=jnp.float32)
    expert_logits = jnp.dot(expert_in, expert_router, preferred_element_type=jnp.float32)
    chosen = expert_ids[:, 0] // per_group
    group_hit = (
        jnp.arange(group_logits.shape[1], dtype=jnp.int32)[None, :] == chosen[:, None]
    ).astype(jnp.float32)
    chosen_logit = jnp.sum(group_logits * group_hit, axis=1, keepdims=True)
    group_share = 1.0 / jnp.sum(jnp.exp(group_logits - chosen_logit), axis=1)
    expert_hit = (
        expert_ids[:, :, None] == jnp.arange(expert_logits.shape[1], dtype=jnp.int32)[None, None, :]
    ).astype(jnp.float32)
    picked_logit = jnp.sum(expert_hit * expert_logits[:, None, :], axis=2)
    inner_share = 1.0 / jnp.sum(
        jnp.exp(picked_logit[:, None, :] - picked_logit[:, :, None]), axis=2
    )
    return group_share[:, None] * inner_share


def on_device(
    residual,
    cache_latent,
    cache_rope,
    lengths,
    query_latent,
    query_rope,
    norm_gain,
    latent_weight,
    latent_gain,
    rope_weight,
    value_weight,
    out_weight,
    mixer_gain,
    group_router,
    expert_router,
    expert_ids,
    gate_weight,
    up_weight,
    down_weight,
):
    ep_count = lax.axis_size("ep")
    seq_count = cache_latent.shape[0]
    group_rows = residual.shape[0]
    model_width = residual.shape[1]
    resid_f = residual.astype(jnp.float32)
    own_rows = lax.dynamic_slice_in_dim(resid_f, lax.axis_index("tp") * seq_count, seq_count, 0)
    normed = (own_rows * inverse_rms(own_rows) * norm_gain.astype(jnp.float32)).astype(jnp.bfloat16)
    latent_raw = jnp.dot(normed, latent_weight, preferred_element_type=jnp.float32)
    new_latent = (latent_raw * inverse_rms(latent_raw) * latent_gain.astype(jnp.float32)).astype(
        jnp.bfloat16
    )
    positions = lengths.astype(jnp.float32)
    rope_raw = jnp.dot(normed, rope_weight.T, preferred_element_type=jnp.float32)
    new_rope_key = rotate(rope_raw, positions).astype(jnp.bfloat16)
    query_turned = rotate(query_rope.astype(jnp.float32), positions[:, None]).astype(jnp.bfloat16)
    score_scale = (NOPE + ROPE) ** (-0.5)
    cached = (
        jnp.einsum("shc,spc->shp", query_latent, cache_latent, preferred_element_type=jnp.float32)
        + jnp.einsum("shr,srp->shp", query_turned, cache_rope, preferred_element_type=jnp.float32)
    ) * score_scale
    keeping = (
        jnp.arange(cache_latent.shape[1], dtype=jnp.int32)[None, None, :] < lengths[:, None, None]
    )
    cached = jnp.where(keeping, cached, -jnp.inf)
    fresh = (
        jnp.einsum("shc,sc->sh", query_latent, new_latent, preferred_element_type=jnp.float32)
        + jnp.einsum("shr,sr->sh", query_turned, new_rope_key, preferred_element_type=jnp.float32)
    ) * score_scale
    row_top = jnp.maximum(jnp.max(cached, axis=2), fresh)
    cached_exp = jnp.exp(cached - row_top[:, :, None])
    fresh_exp = jnp.exp(fresh - row_top)
    denominator = jnp.sum(cached_exp, axis=2) + fresh_exp
    cached_weight = (cached_exp / denominator[:, :, None]).astype(jnp.bfloat16)
    fresh_weight = (fresh_exp / denominator).astype(jnp.bfloat16)
    mixed_latent = (
        jnp.einsum("shp,spc->shc", cached_weight, cache_latent, preferred_element_type=jnp.float32)
        + fresh_weight.astype(jnp.float32)[:, :, None] * new_latent.astype(jnp.float32)[:, None, :]
    ).astype(jnp.bfloat16)
    head_values = jnp.einsum(
        "shc,chv->shv",
        mixed_latent,
        value_weight.reshape(KV, H, V),
        preferred_element_type=jnp.float32,
    ).astype(jnp.bfloat16)
    tp_count = lax.axis_size("tp")
    share_width = model_width // tp_count
    experts = expert_router.shape[1]
    per_group = experts // GROUPS
    local_experts = gate_weight.shape[0]
    capacity = 2 * group_rows * TOPK // experts
    whole_groups = per_group == TOPK and local_experts == TOPK
    slots = capacity if whole_groups else capacity * local_experts
    first_column = lax.axis_index("tp") * share_width
    first_expert = lax.axis_index("ep") * local_experts

    heads = gather_copies(head_values.reshape(seq_count, -1), "tp").reshape(group_rows, -1)
    out_columns = lax.all_to_all(out_weight, "tp", split_axis=1, concat_axis=0, tiled=True)
    attended = jnp.dot(heads, out_columns, preferred_element_type=jnp.float32)
    resid_columns = lax.dynamic_slice_in_dim(residual, first_column, share_width, 1)
    after_columns = (resid_columns.astype(jnp.float32) + attended).astype(jnp.bfloat16)

    sel = slot_table(expert_ids, ep_count, local_experts, slots)
    if whole_groups:
        slot_ids = first_expert + jnp.broadcast_to(
            jnp.arange(TOPK, dtype=jnp.int32)[None], (ep_count * slots, TOPK)
        )
    else:
        all_ids = lax.all_gather(expert_ids, "ep")
        all_sel = jax.vmap(lambda ids: slot_table(ids, ep_count, local_experts, slots))(all_ids)
        mine = lax.dynamic_index_in_dim(all_sel, lax.axis_index("ep"), 1, keepdims=False)
        slot_ids = jnp.einsum(
            "esr,erk->esk", mine, all_ids.astype(jnp.float32), precision=lax.Precision.HIGHEST
        )
        slot_ids = slot_ids.astype(jnp.int32).reshape(-1, TOPK)
    sent = jnp.dot(
        sel.reshape(-1, group_rows).astype(jnp.bfloat16),
        after_columns,
        preferred_element_type=jnp.float32,
    ).astype(jnp.bfloat16)
    sent = jnp.broadcast_to(
        sent.reshape(ep_count, 1, slots, share_width), (ep_count, tp_count, slots, share_width)
    )
    came = lax.all_to_all(
        sent.reshape(-1, slots, share_width), ("ep", "tp"), split_axis=0, concat_axis=0, tiled=True
    )
    rows_f = (
        came.reshape(ep_count, tp_count, slots, share_width)
        .transpose(0, 2, 1, 3)
        .reshape(-1, model_width)
        .astype(jnp.float32)
    )
    expert_in = (rows_f * inverse_rms(rows_f) * mixer_gain.astype(jnp.float32)).astype(jnp.bfloat16)
    route_weight = route_weights(expert_in, group_router, expert_router, slot_ids, per_group)
    local = first_expert + jnp.arange(local_experts, dtype=jnp.int32)
    row_weight = jnp.sum(
        (slot_ids[:, :, None] == local[None, None, :]) * route_weight[:, :, None], axis=1
    )
    gate_value = jnp.einsum("rd,edf->erf", expert_in, gate_weight, preferred_element_type=jnp.float32)
    up_value = jnp.einsum("rd,edf->erf", expert_in, up_weight, preferred_element_type=jnp.float32)
    activation = (jax.nn.silu(gate_value) * up_value).astype(jnp.bfloat16)
    expert_terms = jnp.einsum(
        "erf,efd->erd", activation, down_weight, preferred_element_type=jnp.float32
    )
    row_terms = jnp.sum(expert_terms * row_weight.T[:, :, None], axis=0).astype(jnp.bfloat16)
    back = lax.all_to_all(
        row_terms.reshape(ep_count, slots, tp_count, share_width)
        .transpose(0, 2, 1, 3)
        .reshape(-1, slots, share_width),
        ("ep", "tp"),
        split_axis=0,
        concat_axis=0,
        tiled=True,
    )
    slot_sums = jnp.sum(
        back.reshape(ep_count, tp_count, slots, share_width).astype(jnp.float32), axis=1
    ).reshape(-1, share_width)
    moe_part = jnp.dot(
        sel.reshape(-1, group_rows).T, slot_sums, precision=lax.Precision.HIGHEST
    )
    mixed_share = (after_columns.astype(jnp.float32) + moe_part).astype(jnp.bfloat16)
    mixed = gather_copies(mixed_share, "tp").transpose(1, 0, 2).reshape(group_rows, model_width)
    return (mixed, new_latent, new_rope_key)


def solution(mesh):
    in_specs = (
        P("ep", None),
        P(("ep", "tp"), None, None),
        P(("ep", "tp"), None, None),
        P(("ep", "tp")),
        P(("ep", "tp"), None, None),
        P(("ep", "tp"), None, None),
        P(),
        P(),
        P(),
        P(),
        P(),
        P("tp", None),
        P(),
        P(),
        P(),
        P("ep", None),
        P("ep", None, "tp"),
        P("ep", None, "tp"),
        P("ep", "tp", None),
    )
    out_specs = (P("ep", None), P(("ep", "tp"), None), P(("ep", "tp"), None))
    return jax.shard_map(
        on_device, mesh=mesh, in_specs=in_specs, out_specs=out_specs, check_vma=False
    )
```

```python
import functools

import jax
import jax.numpy as jnp
from jax import lax
from jax.experimental import pallas as pl
from jax.experimental.pallas import tpu as pltpu
from jax.sharding import PartitionSpec as P

H = 32
KV = 256
ROPE = 32
NOPE = 64
V = 64
GROUPS = 4
TOPK = 2


NORM_EPSILON = 1e-06
ROPE_BASE = 10000.0
F32 = jnp.float32
BF16 = jnp.bfloat16
VMEM = pl.BlockSpec(memory_space=pltpu.VMEM)
SMEM = pl.BlockSpec(memory_space=pltpu.SMEM)
HBM = pl.BlockSpec(memory_space=pltpu.HBM)


def inverse_rms(values):
    return lax.rsqrt(jnp.mean(values * values, axis=-1, keepdims=True) + NORM_EPSILON)


def iota(shape, dim):
    return lax.broadcasted_iota(jnp.int32, shape, dim)


def dot(a, b, dims=((1,), (0,)), precision=None):
    return lax.dot_general(a, b, (dims, ((), ())), precision=precision, preferred_element_type=F32)


NT = ((1,), (1,))


def attention_kernel(
    lengths,
    residual_hbm,
    query_latent_hbm,
    query_rope_hbm,
    norm_gain_hbm,
    latent_gain_hbm,
    rope_weight_hbm,
    latent_weight_hbm,
    value_weight_hbm,
    cache_latent_hbm,
    cache_rope_hbm,
    heads_out,
    new_latent_out,
    new_rope_out,
    residual,
    query_latent,
    query_rope,
    norm_gain,
    latent_gain,
    rope_weight,
    latent_weight,
    value_weight,
    cache_latent,
    cache_rope,
    mixed,
    head_rows,
    sems,
):
    seqs = cache_latent.shape[0]
    rows = residual.shape[0]
    loads = []

    def load(source, target):
        copy = pltpu.make_async_copy(source, target, sems.at[len(loads)])
        loads.append(copy)
        copy.start()
        return copy

    latent_loads, rope_loads = [], []
    own_loads = [
        load(residual_hbm, residual),
        load(norm_gain_hbm, norm_gain),
        load(rope_weight_hbm, rope_weight),
        load(latent_gain_hbm, latent_gain),
        load(query_latent_hbm, query_latent),
        load(query_rope_hbm, query_rope),
    ]
    weight_load = load(latent_weight_hbm, latent_weight)
    for s in range(seqs):
        latent_loads.append(load(cache_latent_hbm.at[s], cache_latent.at[s]))
        rope_loads.append(load(cache_rope_hbm.at[s], cache_rope.at[s]))
    value_load = load(value_weight_hbm, value_weight)

    lane = iota((1, ROPE), 1)
    half = ROPE // 2
    low = lane < half
    step = jnp.where(low, lane, lane - half)
    frequency = jnp.zeros((1, ROPE), F32)
    for i in range(half):
        frequency = jnp.where(step == i, F32(ROPE_BASE ** (-2.0 * i / ROPE)), frequency)
    seq_row = iota((seqs, ROPE), 0)
    position = jnp.zeros((seqs, ROPE), F32)
    for s in range(seqs):
        position = jnp.where(seq_row == s, lengths[s].astype(F32), position)
    angles = position * frequency
    cosine = jnp.cos(angles)
    sine = jnp.sin(angles) * jnp.where(low, F32(-1), F32(1))

    for copy in own_loads:
        copy.wait()
    first = lax.axis_index("tp") * seqs
    own_pick = (iota((seqs, rows), 1) == iota((seqs, rows), 0) + first).astype(BF16)
    own = dot(own_pick, residual[...])
    normed = (own * inverse_rms(own) * norm_gain[...].astype(F32)[None, :]).astype(BF16)
    rope_rows = rope_weight[...]
    rope_swapped = jnp.concatenate([rope_rows[half:], rope_rows[:half]], axis=0)
    rope_key = dot(normed, rope_rows, NT) * cosine + dot(normed, rope_swapped, NT) * sine
    rope_key = rope_key.astype(BF16)
    new_rope_out[...] = rope_key
    weight_load.wait()
    latent_raw = dot(normed, latent_weight[...])
    new_latent = latent_raw * inverse_rms(latent_raw) * latent_gain[...].astype(F32)[None, :]
    new_latent = new_latent.astype(BF16)
    new_latent_out[...] = new_latent

    swap = (iota((ROPE, ROPE), 0) == (iota((ROPE, ROPE), 1) + half) % ROPE).astype(BF16)
    scale = (NOPE + ROPE) ** (-0.5)
    for s in range(seqs):
        turning = query_rope[s]
        turned = turning.astype(F32) * cosine[s : s + 1] + dot(turning, swap) * sine[s : s + 1]
        turned = turned.astype(BF16)
        query = query_latent[s]
        fresh_latent = new_latent[s : s + 1].astype(F32)
        fresh_rope = rope_key[s : s + 1].astype(F32)
        fresh = (
            jnp.sum(query.astype(F32) * fresh_latent, axis=1, keepdims=True)
            + jnp.sum(turned.astype(F32) * fresh_rope, axis=1, keepdims=True)
        ) * scale
        latent_loads[s].wait()
        score = dot(query, cache_latent[s], NT)
        rope_loads[s].wait()
        score = (score + dot(turned, cache_rope[s])) * scale
        score = jnp.where(iota(score.shape, 1) < lengths[s], score, -jnp.inf)
        top = jnp.maximum(jnp.max(score, axis=1, keepdims=True), fresh)
        score = jnp.exp(score - top)
        fresh = jnp.exp(fresh - top)
        share = 1.0 / (jnp.sum(score, axis=1, keepdims=True) + fresh)
        weight = (score * share).astype(BF16)
        fresh = (fresh * share).astype(BF16).astype(F32)
        mix = dot(weight, cache_latent[s]) + fresh * fresh_latent
        mixed[s * H : (s + 1) * H, :] = mix.astype(BF16)

    value_load.wait()
    spread = dot(mixed[...], value_weight[...])
    first = iota((H, H * V), 0) * V
    column = iota((H, H * V), 1)
    own_head = (column >= first) & (column < first + V)
    for s in range(seqs):
        kept = jnp.where(own_head, spread[s * H : (s + 1) * H], F32(0))
        head_rows[s : s + 1, :] = jnp.sum(kept, axis=0, keepdims=True)
    shares, _, width = heads_out.shape
    for t in range(shares):
        heads_out[t] = head_rows[:, t * width : (t + 1) * width].astype(BF16)


def attention(
    lengths, residual, query_latent, query_rope, norm_gain, latent_gain, rope_weight,
    latent_weight, value_weight, cache_latent, cache_rope, shares,
):
    seqs, cached, _ = cache_latent.shape
    width = H * V // shares
    return pl.pallas_call(
        attention_kernel,
        name="attention",
        out_shape=(
            jax.ShapeDtypeStruct((shares, seqs, width), BF16),
            jax.ShapeDtypeStruct((seqs, KV), BF16),
            jax.ShapeDtypeStruct((seqs, ROPE), BF16),
        ),
        in_specs=[SMEM] + [HBM] * 10,
        out_specs=(VMEM, VMEM, VMEM),
        scratch_shapes=[
            pltpu.VMEM(residual.shape, BF16),
            pltpu.VMEM(query_latent.shape, BF16),
            pltpu.VMEM(query_rope.shape, BF16),
            pltpu.VMEM(norm_gain.shape, BF16),
            pltpu.VMEM(latent_gain.shape, BF16),
            pltpu.VMEM(rope_weight.shape, BF16),
            pltpu.VMEM(latent_weight.shape, BF16),
            pltpu.VMEM(value_weight.shape, BF16),
            pltpu.VMEM(cache_latent.shape, BF16),
            pltpu.VMEM(cache_rope.shape, BF16),
            pltpu.VMEM((seqs * H, KV), BF16),
            pltpu.VMEM((seqs, H * V), F32),
            pltpu.SemaphoreType.DMA((2 * seqs + 8,)),
        ],
        cost_estimate=pl.CostEstimate(
            flops=2 * seqs * H * cached * (2 * KV + ROPE), bytes_accessed=8 * 2**20, transcendentals=0
        ),
    )(
        lengths, residual, query_latent, query_rope, norm_gain, latent_gain, rope_weight,
        latent_weight, value_weight, cache_latent, cache_rope,
    )


def project_kernel(heads, out_weight, terms_out, gathered):
    shares, seqs, _ = heads.shape
    for t in range(shares):
        gathered[t * seqs : (t + 1) * seqs, :] = heads[t].astype(F32)
    terms = dot(gathered[...].astype(BF16), out_weight[...])
    width = terms_out.shape[2]
    for t in range(shares):
        terms_out[t] = terms[:, t * width : (t + 1) * width].astype(BF16)


def project(heads, out_weight):
    shares, seqs, width = heads.shape
    columns = out_weight.shape[1]
    return pl.pallas_call(
        project_kernel,
        name="project",
        out_shape=jax.ShapeDtypeStruct((shares, shares * seqs, columns // shares), BF16),
        in_specs=[VMEM, VMEM],
        out_specs=VMEM,
        scratch_shapes=[pltpu.VMEM((shares * seqs, width), F32)],
        compiler_params=pltpu.CompilerParams(vmem_limit_bytes=8 * 2**20),
        cost_estimate=pl.CostEstimate(
            flops=2 * shares * seqs * width * columns, bytes_accessed=2**20, transcendentals=0
        ),
    )(heads, out_weight)


def dispatch_kernel(local_experts, slots, terms, residual, expert_ids, sent_out, after_out, pick_out):
    shares, rows, width = terms.shape
    total = terms[0].astype(F32)
    for t in range(1, shares):
        total = total + terms[t].astype(F32)
    first = pl.multiple_of(lax.axis_index("tp") * width, width)
    ep_count = sent_out.shape[0] // shares
    after = (residual[:, pl.ds(first, width)].astype(F32) + total).astype(BF16)
    after_out[...] = after

    index = iota((ep_count, rows), 0) * local_experts
    hit = None
    for k in range(TOPK):
        named = expert_ids[k : k + 1, :]
        here = (named >= index) & (named < index + local_experts)
        hit = here if hit is None else hit | here
    hit = hit.astype(F32)
    earlier = (iota((rows, rows), 0) < iota((rows, rows), 1)).astype(BF16)
    rank = dot(hit.astype(BF16), earlier)
    rank = jnp.where(hit > 0.5, rank, F32(-1))
    slot = iota((slots, rows), 0).astype(F32)
    for e in range(ep_count):
        pick = (rank[e : e + 1, :] == slot).astype(F32)
        pick_out[e * slots : (e + 1) * slots, :] = pick
    chosen = dot(pick_out[...].astype(BF16), after).astype(BF16)
    for e in range(ep_count):
        for t in range(shares):
            sent_out[e * shares + t] = chosen[e * slots : (e + 1) * slots]


def dispatch(terms, residual, expert_ids, ep_count, local_experts, slots):
    shares, rows, width = terms.shape
    return pl.pallas_call(
        functools.partial(dispatch_kernel, local_experts, slots),
        name="dispatch",
        out_shape=(
            jax.ShapeDtypeStruct((ep_count * shares, slots, width), BF16),
            jax.ShapeDtypeStruct((rows, width), BF16),
            jax.ShapeDtypeStruct((ep_count * slots, rows), F32),
        ),
        in_specs=[VMEM] * 3,
        out_specs=(VMEM, VMEM, VMEM),
        compiler_params=pltpu.CompilerParams(vmem_limit_bytes=8 * 2**20),
        cost_estimate=pl.CostEstimate(flops=10**6, bytes_accessed=2**20, transcendentals=0),
    )(terms, residual, expert_ids)


def experts_kernel(
    shares, came, mixer_gain, group_router, expert_router, choice, gate_hbm, up_hbm, down_hbm,
    back_out, rows_in, gate, up, down, sems,
):
    loads = []
    for l in range(gate.shape[0]):
        for n, (source, target) in enumerate(((gate_hbm, gate), (up_hbm, up), (down_hbm, down))):
            copy = pltpu.make_async_copy(source.at[l], target.at[l], sems.at[3 * l + n])
            copy.start()
            loads.append(copy)
    ep_count = came.shape[0] // shares
    _, slots, width = came.shape
    for e in range(ep_count):
        for t in range(shares):
            rows_in[e * slots : (e + 1) * slots, t * width : (t + 1) * width] = came[e * shares + t]
    after = rows_in[...].astype(F32)
    expert_in = (after * inverse_rms(after) * mixer_gain[...].astype(F32)[None, :]).astype(BF16)

    group_logits = dot(expert_in, group_router[...], NT)
    expert_logits = dot(expert_in, expert_router[...], NT)
    choices = choice[...]
    group_hit = iota(group_logits.shape, 1) == choices[:, 2 * TOPK : 2 * TOPK + 1]
    own_group = jnp.sum(jnp.where(group_hit, group_logits, F32(0)), axis=1, keepdims=True)
    group_share = 1.0 / jnp.sum(jnp.exp(group_logits - own_group), axis=1, keepdims=True)
    picked = []
    for k in range(TOPK):
        expert_hit = iota(expert_logits.shape, 1) == choices[:, k : k + 1]
        picked.append(jnp.sum(jnp.where(expert_hit, expert_logits, F32(0)), axis=1, keepdims=True))
    route = []
    for k in range(TOPK):
        total = jnp.exp(picked[0] - picked[k])
        for j in range(1, TOPK):
            total = total + jnp.exp(picked[j] - picked[k])
        route.append(group_share / total)

    result = None
    for l in range(gate.shape[0]):
        weight = jnp.where(choices[:, TOPK : TOPK + 1] == l, route[0], F32(0))
        for k in range(1, TOPK):
            weight = weight + jnp.where(choices[:, TOPK + k : TOPK + k + 1] == l, route[k], F32(0))
        loads[3 * l].wait()
        gated = dot(expert_in, gate[l])
        loads[3 * l + 1].wait()
        raised = dot(expert_in, up[l])
        act = (gated / (1.0 + jnp.exp(-gated)) * raised).astype(BF16)
        loads[3 * l + 2].wait()
        part = dot(act, down[l]) * weight
        result = part if result is None else result + part
    result = result.astype(BF16)
    for e in range(ep_count):
        for t in range(shares):
            back_out[e * shares + t] = result[e * slots : (e + 1) * slots, t * width : (t + 1) * width]


def run_experts(came, mixer_gain, group_router, expert_router, choice, gate, up, down, shares):
    count, slots, width = came.shape
    rows, model = count // shares * slots, shares * width
    return pl.pallas_call(
        functools.partial(experts_kernel, shares),
        name="experts",
        out_shape=jax.ShapeDtypeStruct(came.shape, BF16),
        in_specs=[VMEM] * 5 + [HBM] * 3,
        out_specs=VMEM,
        scratch_shapes=[
            pltpu.VMEM((rows, model), BF16),
            pltpu.VMEM(gate.shape, BF16),
            pltpu.VMEM(up.shape, BF16),
            pltpu.VMEM(down.shape, BF16),
            pltpu.SemaphoreType.DMA((3 * gate.shape[0],)),
        ],
        cost_estimate=pl.CostEstimate(
            flops=6 * rows * gate.size, bytes_accessed=6 * gate.size, transcendentals=0
        ),
    )(came, mixer_gain, group_router, expert_router, choice, gate, up, down)


def combine_kernel(shares, back, pick, after, copies_out, sums):
    count, slots, _ = back.shape
    for e in range(count // shares):
        total = back[e * shares].astype(F32)
        for t in range(1, shares):
            total = total + back[e * shares + t].astype(F32)
        sums[e * slots : (e + 1) * slots, :] = total
    moe = dot(pick[...], sums[...], ((0,), (0,)), lax.Precision.HIGHEST)
    mixed = (after[...].astype(F32) + moe).astype(BF16)
    for t in range(shares):
        copies_out[t] = mixed


def combine(back, pick, after, shares):
    count, slots, width = back.shape
    return pl.pallas_call(
        functools.partial(combine_kernel, shares),
        name="combine",
        out_shape=jax.ShapeDtypeStruct((shares,) + after.shape, BF16),
        in_specs=[VMEM] * 3,
        out_specs=VMEM,
        scratch_shapes=[pltpu.VMEM((count // shares * slots, width), F32)],
        compiler_params=pltpu.CompilerParams(vmem_limit_bytes=8 * 2**20),
        cost_estimate=pl.CostEstimate(flops=10**6, bytes_accessed=2**20, transcendentals=0),
    )(back, pick, after)


def exchange(blocks, axis):
    return lax.all_to_all(blocks, axis, split_axis=0, concat_axis=0, tiled=True)


def slot_owners(expert_ids, local_experts):
    return (expert_ids // local_experts).T


def slot_table(owners, index, slots):
    hit = jnp.any(owners == index, axis=0).astype(jnp.int32)
    rank = jnp.cumsum(hit) - hit
    return (rank[None, :] == jnp.arange(slots)[:, None]) & (hit[None, :] > 0)


def on_device(
    residual,
    cache_latent,
    cache_rope,
    lengths,
    query_latent,
    query_rope,
    norm_gain,
    latent_weight,
    latent_gain,
    rope_weight,
    value_weight,
    out_weight,
    mixer_gain,
    group_router,
    expert_router,
    expert_ids,
    gate_weight,
    up_weight,
    down_weight,
):
    ep_count = lax.axis_size("ep")
    tp_count = lax.axis_size("tp")
    group_rows, model_width = residual.shape
    experts = expert_router.shape[1]
    per_group = experts // GROUPS
    local_experts = gate_weight.shape[0]
    capacity = 2 * group_rows * TOPK // experts
    whole_groups = per_group == TOPK and local_experts == TOPK
    slots = capacity if whole_groups else capacity * local_experts
    first_expert = lax.axis_index("ep") * local_experts
    if whole_groups:
        slot_ids = jnp.broadcast_to(
            first_expert + jnp.arange(TOPK, dtype=jnp.int32)[None], (ep_count * slots, TOPK)
        )
    else:
        all_ids = lax.all_gather(expert_ids, "ep")
        mine = jax.vmap(
            lambda ids: slot_table(slot_owners(ids, local_experts), lax.axis_index("ep"), slots)
        )(all_ids)
        slot_ids = jnp.sum(
            mine[:, :, :, None].astype(jnp.int32) * all_ids[:, None, :, :], axis=2
        ).reshape(-1, TOPK)
    choice = jnp.concatenate(
        [slot_ids, slot_ids - first_expert, slot_ids[:, :1] // per_group], axis=1
    )

    heads, new_latent, new_rope_key = attention(
        lengths, residual, query_latent, query_rope, norm_gain, latent_gain,
        rope_weight, latent_weight, value_weight, cache_latent, cache_rope, tp_count,
    )
    terms = project(exchange(heads, "tp"), out_weight)
    sent, after, pick = dispatch(
        exchange(terms, "tp"), residual, expert_ids.T, ep_count, local_experts, slots
    )
    back = run_experts(
        exchange(sent, ("ep", "tp")), mixer_gain, group_router.T, expert_router.T, choice,
        gate_weight, up_weight, down_weight, tp_count,
    )
    copies = combine(exchange(back, ("ep", "tp")), pick, after, tp_count)
    mixed = exchange(copies, "tp").transpose(1, 0, 2).reshape(group_rows, model_width)
    return (mixed, new_latent, new_rope_key)


def solution(mesh):
    in_specs = (
        P("ep", None),
        P(("ep", "tp"), None, None),
        P(("ep", "tp"), None, None),
        P(("ep", "tp")),
        P(("ep", "tp"), None, None),
        P(("ep", "tp"), None, None),
        P(),
        P(),
        P(),
        P(),
        P(),
        P("tp", None),
        P(),
        P(),
        P(),
        P("ep", None),
        P("ep", None, "tp"),
        P("ep", None, "tp"),
        P("ep", "tp", None),
    )
    out_specs = (P("ep", None), P(("ep", "tp"), None), P(("ep", "tp"), None))
    return jax.shard_map(
        on_device, mesh=mesh, in_specs=in_specs, out_specs=out_specs, check_vma=False
    )
```

```python
import functools

import jax
import jax.numpy as jnp
from jax import lax
from jax.experimental import pallas as pl
from jax.experimental.pallas import tpu as pltpu
from jax.sharding import PartitionSpec as P

H = 32
KV = 256
ROPE = 32
NOPE = 64
V = 64
GROUPS = 4
TOPK = 2
CORES = 2
LARGE = 24


NORM_EPSILON = 1e-06
ROPE_BASE = 10000.0
F32 = jnp.float32
BF16 = jnp.bfloat16
VMEM = pl.BlockSpec(memory_space=pltpu.VMEM)
SMEM = pl.BlockSpec(memory_space=pltpu.SMEM)
HBM = pl.BlockSpec(memory_space=pltpu.HBM)


def inverse_rms(values):
    return lax.rsqrt(jnp.mean(values * values, axis=-1, keepdims=True) + NORM_EPSILON)


def iota(shape, dim):
    return lax.broadcasted_iota(jnp.int32, shape, dim)


def dot(a, b, dims=((1,), (0,)), precision=None):
    return lax.dot_general(a, b, (dims, ((), ())), precision=precision, preferred_element_type=F32)


NT = ((1,), (1,))


def attention_kernel(
    lengths_hbm,
    residual_hbm,
    query_latent_hbm,
    query_rope_hbm,
    norm_gain_hbm,
    latent_gain_hbm,
    rope_weight_hbm,
    latent_weight_hbm,
    value_weight_hbm,
    cache_latent_hbm,
    cache_rope_hbm,
    heads_out,
    new_latent_hbm,
    new_rope_hbm,
    lengths,
    new_latent_out,
    new_rope_out,
    residual,
    query_latent,
    query_rope,
    norm_gain,
    latent_gain,
    rope_weight,
    latent_weight,
    value_weight,
    cache_latent,
    cache_rope,
    mixed,
    head_rows,
    sems,
):
    seqs = cache_latent.shape[0]
    rows = residual.shape[0]
    loads = []

    def load(source, target):
        copy = pltpu.make_async_copy(source, target, sems.at[len(loads)])
        loads.append(copy)
        copy.start()
        return copy

    latent_loads, rope_loads = [], []
    length_load = load(lengths_hbm, lengths)
    own_loads = [
        load(residual_hbm, residual),
        load(norm_gain_hbm, norm_gain),
        load(rope_weight_hbm, rope_weight),
        load(latent_gain_hbm, latent_gain),
        load(query_latent_hbm, query_latent),
        load(query_rope_hbm, query_rope),
    ]
    weight_load = load(latent_weight_hbm, latent_weight)
    for s in range(seqs):
        latent_loads.append(load(cache_latent_hbm.at[s], cache_latent.at[s]))
        rope_loads.append(load(cache_rope_hbm.at[s], cache_rope.at[s]))
    value_load = load(value_weight_hbm, value_weight)

    lane = iota((1, ROPE), 1)
    half = ROPE // 2
    low = lane < half
    step = jnp.where(low, lane, lane - half)
    frequency = jnp.zeros((1, ROPE), F32)
    for i in range(half):
        frequency = jnp.where(step == i, F32(ROPE_BASE ** (-2.0 * i / ROPE)), frequency)
    seq_row = iota((seqs, ROPE), 0)
    length_load.wait()
    position = jnp.zeros((seqs, ROPE), F32)
    for s in range(seqs):
        position = jnp.where(seq_row == s, lengths[s].astype(F32), position)
    angles = position * frequency
    cosine = jnp.cos(angles)
    sine = jnp.sin(angles) * jnp.where(low, F32(-1), F32(1))

    for copy in own_loads:
        copy.wait()
    first = lax.axis_index("tp") * seqs
    own_pick = (iota((seqs, rows), 1) == iota((seqs, rows), 0) + first).astype(BF16)
    own = dot(own_pick, residual[...])
    normed = (own * inverse_rms(own) * norm_gain[...].astype(F32)[None, :]).astype(BF16)
    rope_rows = rope_weight[...]
    rope_swapped = jnp.concatenate([rope_rows[half:], rope_rows[:half]], axis=0)
    rope_key = dot(normed, rope_rows, NT) * cosine + dot(normed, rope_swapped, NT) * sine
    rope_key = rope_key.astype(BF16)
    new_rope_out[...] = rope_key
    rope_store = load(new_rope_out, new_rope_hbm)
    weight_load.wait()
    latent_raw = dot(normed, latent_weight[...])
    new_latent = latent_raw * inverse_rms(latent_raw) * latent_gain[...].astype(F32)[None, :]
    new_latent = new_latent.astype(BF16)
    new_latent_out[...] = new_latent
    latent_store = load(new_latent_out, new_latent_hbm)

    swap = (iota((ROPE, ROPE), 0) == (iota((ROPE, ROPE), 1) + half) % ROPE).astype(BF16)
    scale = (NOPE + ROPE) ** (-0.5)
    for s in range(seqs):
        turning = query_rope[s]
        turned = turning.astype(F32) * cosine[s : s + 1] + dot(turning, swap) * sine[s : s + 1]
        turned = turned.astype(BF16)
        query = query_latent[s]
        fresh_latent = new_latent[s : s + 1].astype(F32)
        fresh_rope = rope_key[s : s + 1].astype(F32)
        fresh = (
            jnp.sum(query.astype(F32) * fresh_latent, axis=1, keepdims=True)
            + jnp.sum(turned.astype(F32) * fresh_rope, axis=1, keepdims=True)
        ) * scale
        latent_loads[s].wait()
        score = dot(query, cache_latent[s], NT)
        rope_loads[s].wait()
        score = (score + dot(turned, cache_rope[s])) * scale
        score = jnp.where(iota(score.shape, 1) < lengths[s], score, -jnp.inf)
        top = jnp.maximum(jnp.max(score, axis=1, keepdims=True), fresh)
        score = jnp.exp(score - top)
        fresh = jnp.exp(fresh - top)
        share = 1.0 / (jnp.sum(score, axis=1, keepdims=True) + fresh)
        weight = (score * share).astype(BF16)
        fresh = (fresh * share).astype(BF16).astype(F32)
        mix = dot(weight, cache_latent[s]) + fresh * fresh_latent
        mixed[s * H : (s + 1) * H, :] = mix.astype(BF16)

    value_load.wait()
    spread = dot(mixed[...], value_weight[...])
    first = iota((H, H * V), 0) * V
    column = iota((H, H * V), 1)
    own_head = (column >= first) & (column < first + V)
    for s in range(seqs):
        kept = jnp.where(own_head, spread[s * H : (s + 1) * H], F32(0))
        head_rows[s : s + 1, :] = jnp.sum(kept, axis=0, keepdims=True)
    shares, _, width = heads_out.shape
    for t in range(shares):
        chip = t // CORES
        heads_out[t] = head_rows[:, chip * width : (chip + 1) * width].astype(BF16)
    rope_store.wait()
    latent_store.wait()


def attention(
    lengths, residual, query_latent, query_rope, norm_gain, latent_gain, rope_weight,
    latent_weight, value_weight, cache_latent, cache_rope, shares,
):
    seqs, cached, _ = cache_latent.shape
    width = H * V * CORES // shares
    in_hbm = [
        pltpu.with_memory_space_constraint(a, pltpu.HBM)
        for a in (
            lengths, residual, query_latent, query_rope, norm_gain, latent_gain, rope_weight,
            latent_weight, value_weight, cache_latent, cache_rope,
        )
    ]
    return pl.pallas_call(
        attention_kernel,
        name="attention",
        out_shape=(
            jax.ShapeDtypeStruct((shares, seqs, width), BF16),
            jax.ShapeDtypeStruct((seqs, KV), BF16),
            jax.ShapeDtypeStruct((seqs, ROPE), BF16),
        ),
        in_specs=[HBM] * 11,
        out_specs=(VMEM, HBM, HBM),
        scratch_shapes=[
            pltpu.SMEM(lengths.shape, jnp.int32),
            pltpu.VMEM((seqs, KV), BF16),
            pltpu.VMEM((seqs, ROPE), BF16),
            pltpu.VMEM(residual.shape, BF16),
            pltpu.VMEM(query_latent.shape, BF16),
            pltpu.VMEM(query_rope.shape, BF16),
            pltpu.VMEM(norm_gain.shape, BF16),
            pltpu.VMEM(latent_gain.shape, BF16),
            pltpu.VMEM(rope_weight.shape, BF16),
            pltpu.VMEM(latent_weight.shape, BF16),
            pltpu.VMEM(value_weight.shape, BF16),
            pltpu.VMEM(cache_latent.shape, BF16),
            pltpu.VMEM(cache_rope.shape, BF16),
            pltpu.VMEM((seqs * H, KV), BF16),
            pltpu.VMEM((seqs, H * V), F32),
            pltpu.SemaphoreType.DMA((2 * seqs + 11,)),
        ],
        compiler_params=pltpu.CompilerParams(vmem_limit_bytes=LARGE * 2**20),
        cost_estimate=pl.CostEstimate(
            flops=2 * seqs * H * cached * (2 * KV + ROPE), bytes_accessed=8 * 2**20, transcendentals=0
        ),
    )(*in_hbm)


def own_half(width):
    core = lax.rem(lax.axis_index("tp"), CORES)
    return pl.multiple_of(core * width, width), pl.multiple_of((1 - core) * width, width)


def tree_sum(terms):
    while len(terms) > 1:
        terms = [terms[i] + terms[i + 1] for i in range(0, len(terms), 2)]
    return terms[0]


def call(kernel, name, out_shape, scratch, operands, **params):
    limit = params.pop("limit", 8)
    flops = params.pop("flops", 10**6)
    moved = params.pop("moved", 2**20)
    return pl.pallas_call(
        kernel,
        name=name,
        out_shape=out_shape,
        scratch_shapes=scratch,
        compiler_params=pltpu.CompilerParams(vmem_limit_bytes=limit * 2**20),
        cost_estimate=pl.CostEstimate(flops=flops, bytes_accessed=moved, transcendentals=0),
        **params,
    )(*operands)


def shaped(shape, dtype=BF16):
    return jax.ShapeDtypeStruct(shape, dtype)


def project_kernel(heads, own_weight, other_weight, terms_out, gathered):
    shares, seqs, _ = heads.shape
    for t in range(shares):
        gathered[t * seqs : (t + 1) * seqs, :] = heads[t].astype(F32)
    own_rows, other_rows = own_half(own_weight.shape[0])
    width = terms_out.shape[1]
    columns = pl.ds(own_half(width)[0], width)
    terms = dot(
        gathered[:, pl.ds(own_rows, own_weight.shape[0])].astype(BF16), own_weight[:, columns]
    ) + dot(
        gathered[:, pl.ds(other_rows, own_weight.shape[0])].astype(BF16), other_weight[:, columns]
    )
    terms_out[...] = terms.astype(BF16)


def project(heads, own_weight, other_weight):
    shares, seqs, width = heads.shape
    columns = own_weight.shape[1] // CORES
    return call(
        project_kernel, "project", shaped((shares * seqs, columns)),
        [pltpu.VMEM((shares * seqs, width), F32)], (heads, own_weight, other_weight),
        in_specs=[VMEM] * 3, out_specs=VMEM, flops=2 * shares * seqs * width * columns,
    )


def dispatch_kernel(count, local_experts, slots, *refs):
    terms, (residual, expert_ids), outs = refs[:count], refs[count : count + 2], refs[count + 2 :]
    sent_out, (after_out, pick_out) = outs[:-2], outs[-2:]
    rows, width = terms[0].shape
    total = tree_sum([part[...].astype(F32) for part in terms])
    own_columns = pl.ds(own_half(width)[0], width)
    after = (residual[:, own_columns].astype(F32) + total).astype(BF16)
    after_out[...] = after

    ep_count = len(sent_out)
    index = (iota((ep_count, rows), 0) ^ lax.axis_index("ep")) * local_experts
    hit = None
    for k in range(TOPK):
        named = expert_ids[k : k + 1, :]
        here = (named >= index) & (named < index + local_experts)
        hit = here if hit is None else hit | here
    hit = hit.astype(F32)
    earlier = (iota((rows, rows), 0) < iota((rows, rows), 1)).astype(BF16)
    rank = jnp.where(hit > 0.5, dot(hit.astype(BF16), earlier), F32(-1))
    slot = iota((slots, rows), 0).astype(F32)
    pick = jnp.concatenate(
        [(rank[e : e + 1, :] == slot).astype(F32) for e in range(ep_count)], axis=0
    ).astype(BF16)
    pick_out[...] = pick
    chosen = dot(pick, after).astype(BF16)
    for e in range(ep_count):
        sent_out[e][...] = chosen[e * slots : (e + 1) * slots]


def dispatch(terms, residual, expert_ids, ep_count, local_experts, slots):
    rows, width = terms[0].shape
    outs = call(
        functools.partial(dispatch_kernel, len(terms), local_experts, slots), "dispatch",
        (shaped((slots, width)),) * ep_count
        + (shaped((rows, width)), shaped((ep_count * slots, rows))),
        [], (*terms, residual, expert_ids),
        in_specs=[VMEM] * (len(terms) + 2), out_specs=(VMEM,) * (ep_count + 2),
    )
    return outs[:ep_count], outs[ep_count], outs[ep_count + 1]


def experts_kernel(
    own_rows, other_rows, mixer_gain, group_router, expert_router, *refs
):
    *choice, gate, up, down_hbm, keep_out, give_out, rows_in, down, sems = refs
    loads = []
    for l in range(gate.shape[0]):
        loads.append(pltpu.make_async_copy(down_hbm.at[l], down.at[l], sems.at[l]))
        loads[l].start()
    width = own_rows.shape[1]
    own_at, other_at = own_half(width)
    rows_in[:, pl.ds(own_at, width)] = own_rows[...].astype(F32)
    rows_in[:, pl.ds(other_at, width)] = other_rows[...].astype(F32)
    after = rows_in[...]
    expert_in = (after * inverse_rms(after) * mixer_gain[...].astype(F32)[None, :]).astype(BF16)

    group_logits = dot(expert_in, group_router[...], NT)
    expert_logits = dot(expert_in, expert_router[...], NT)
    first = lax.axis_index("ep") * gate.shape[0]
    if choice:
        chosen = choice[0][...]
        ids, group = [chosen[:, k : k + 1] for k in range(TOPK)], chosen[:, TOPK : TOPK + 1]
    else:
        ids, group = [first + k for k in range(TOPK)], lax.axis_index("ep")
    group_hit = iota(group_logits.shape, 1) == group
    own_group = jnp.sum(jnp.where(group_hit, group_logits, F32(0)), axis=1, keepdims=True)
    group_share = 1.0 / jnp.sum(jnp.exp(group_logits - own_group), axis=1, keepdims=True)
    picked = []
    for k in range(TOPK):
        expert_hit = iota(expert_logits.shape, 1) == ids[k]
        picked.append(jnp.sum(jnp.where(expert_hit, expert_logits, F32(0)), axis=1, keepdims=True))
    route = []
    for k in range(TOPK):
        total = jnp.exp(picked[0] - picked[k])
        for j in range(1, TOPK):
            total = total + jnp.exp(picked[j] - picked[k])
        route.append(group_share / total)

    result = None
    for l in range(gate.shape[0]):
        weight = jnp.where(ids[0] == first + l, route[0], F32(0))
        for k in range(1, TOPK):
            weight = weight + jnp.where(ids[k] == first + l, route[k], F32(0))
        gated = dot(expert_in, gate[l])
        raised = dot(expert_in, up[l])
        act = (gated / (1.0 + jnp.exp(-gated)) * raised).astype(BF16)
        loads[l].wait()
        part = dot(act, down[l]) * weight
        result = part if result is None else result + part
    rows_in[...] = result
    keep_out[...] = rows_in[:, pl.ds(own_at, width)]
    give_out[...] = rows_in[:, pl.ds(other_at, width)].astype(BF16)


def run_experts(own_rows, other_rows, mixer_gain, group_router, expert_router, choice, weights):
    rows, width = own_rows.shape
    gate, up, down = weights
    gate = pltpu.with_memory_space_constraint(gate, pltpu.VMEM)
    up = pltpu.with_memory_space_constraint(up, pltpu.VMEM)
    down = pltpu.with_memory_space_constraint(down, pltpu.HBM)
    return call(
        experts_kernel, "experts",
        (shaped((rows, width), F32), shaped((rows, width))),
        [
            pltpu.VMEM((rows, CORES * width), F32),
            pltpu.VMEM(down.shape, BF16),
            pltpu.SemaphoreType.DMA((down.shape[0],)),
        ],
        (own_rows, other_rows, mixer_gain, group_router, expert_router, *choice, gate, up, down),
        in_specs=[VMEM] * (7 + len(choice)) + [HBM], out_specs=(VMEM, VMEM),
        flops=6 * rows * gate.size, moved=6 * gate.size, limit=LARGE,
    )


def fold_kernel(keep, came, *blocks_out):
    total = (keep[...] + came[...].astype(F32)).astype(BF16)
    slots = blocks_out[0].shape[0]
    for e, block in enumerate(blocks_out):
        block[...] = total[e * slots : (e + 1) * slots]


def fold(keep, came, ep_count):
    rows, width = keep.shape
    return call(
        fold_kernel, "fold", (shaped((rows // ep_count, width)),) * ep_count, [], (keep, came),
        in_specs=[VMEM] * 2, out_specs=(VMEM,) * ep_count,
    )


def collect_kernel(pick, *refs):
    *blocks, out = refs
    back = jnp.concatenate([block[...] for block in blocks], axis=0)
    out[...] = dot(pick[...], back, ((0,), (0,))).astype(BF16)


def collect(pick, blocks):
    return call(
        collect_kernel, "collect", shaped((pick.shape[1], blocks[0].shape[1])), [],
        (pick, *blocks), in_specs=[VMEM] * (1 + len(blocks)), out_specs=VMEM,
    )


def mix_kernel(after, *refs):
    *terms, out = refs
    total = tree_sum([part[...].astype(F32) for part in terms])
    out[...] = (after[...].astype(F32) + total).astype(BF16)


def mix(after, terms):
    return call(
        mix_kernel, "mix", shaped(after.shape), [], (after, *terms),
        in_specs=[VMEM] * (1 + len(terms)), out_specs=VMEM,
    )


def place_kernel(own, other, out):
    width = own.shape[1]
    own_at, other_at = own_half(width)
    out[:, pl.ds(own_at, width)] = own[...]
    out[:, pl.ds(other_at, width)] = other[...]


def place_halves(own, other):
    rows, width = own.shape
    return call(
        place_kernel, "place", shaped((rows, CORES * width)), [], (own, other),
        in_specs=[VMEM] * 2, out_specs=VMEM,
    )


def flip(block, axis, bits):
    return lax.ppermute(block, axis, [(i, i ^ bits) for i in range(lax.axis_size(axis))])


def from_chips(block):
    chips = lax.axis_size("tp") // CORES
    return [block] + [flip(block, "tp", CORES * m) for m in range(1, chips)]


def swap_blocks(blocks):
    return [blocks[0]] + [flip(blocks[m], "ep", m) for m in range(1, len(blocks))]


def exchange(blocks, axis):
    return lax.all_to_all(blocks, axis, split_axis=0, concat_axis=0, tiled=True)


def slot_owners(expert_ids, local_experts):
    return (expert_ids // local_experts).T


def slot_table(owners, index, slots):
    hit = jnp.any(owners == index, axis=0).astype(jnp.int32)
    rank = jnp.cumsum(hit) - hit
    return (rank[None, :] == jnp.arange(slots)[:, None]) & (hit[None, :] > 0)


def on_device(
    residual,
    cache_latent,
    cache_rope,
    lengths,
    query_latent,
    query_rope,
    norm_gain,
    latent_weight,
    latent_gain,
    rope_weight,
    value_weight,
    out_weight,
    mixer_gain,
    group_router,
    expert_router,
    expert_ids,
    gate_weight,
    up_weight,
    down_weight,
):
    ep_count = lax.axis_size("ep")
    tp_count = lax.axis_size("tp")
    group_rows, model_width = residual.shape
    experts = expert_router.shape[1]
    per_group = experts // GROUPS
    local_experts = gate_weight.shape[0]
    capacity = 2 * group_rows * TOPK // experts
    whole_groups = per_group == TOPK and local_experts == TOPK
    slots = capacity if whole_groups else capacity * local_experts
    choice = ()
    if not whole_groups:
        here = lax.axis_index("ep")
        order = here ^ jnp.arange(ep_count, dtype=jnp.int32)
        all_ids = jnp.take(lax.all_gather(expert_ids, "ep"), order, axis=0)
        mine = jax.vmap(lambda ids: slot_table(slot_owners(ids, local_experts), here, slots))(all_ids)
        slot_ids = jnp.sum(
            mine[:, :, :, None].astype(jnp.int32) * all_ids[:, None, :, :], axis=2
        ).reshape(-1, TOPK)
        choice = (jnp.concatenate([slot_ids, slot_ids[:, :1] // per_group], axis=1),)

    other_weight = flip(out_weight, "tp", 1)
    heads, new_latent, new_rope_key = attention(
        lengths, residual, query_latent, query_rope, norm_gain, latent_gain,
        rope_weight, latent_weight, value_weight, cache_latent, cache_rope, tp_count,
    )
    terms = project(exchange(heads, "tp"), out_weight, other_weight)
    sent, after, pick = dispatch(
        from_chips(terms), residual, expert_ids.T, ep_count, local_experts, slots
    )
    own_rows = jnp.concatenate(swap_blocks(sent), axis=0)
    keep, give = run_experts(
        own_rows, flip(own_rows, "tp", 1), mixer_gain, group_router.T, expert_router.T, choice,
        (gate_weight, up_weight, down_weight),
    )
    back = swap_blocks(fold(keep, flip(give, "tp", 1), ep_count))
    mixed_half = mix(after, from_chips(collect(pick, back)))
    mixed = place_halves(mixed_half, flip(mixed_half, "tp", 1))
    return (mixed, new_latent, new_rope_key)


def solution(mesh):
    in_specs = (
        P("ep", None),
        P(("ep", "tp"), None, None),
        P(("ep", "tp"), None, None),
        P(("ep", "tp")),
        P(("ep", "tp"), None, None),
        P(("ep", "tp"), None, None),
        P(),
        P(),
        P(),
        P(),
        P(),
        P("tp", None),
        P(),
        P(),
        P(),
        P("ep", None),
        P("ep", None, "tp"),
        P("ep", None, "tp"),
        P("ep", "tp", None),
    )
    out_specs = (P("ep", None), P(("ep", "tp"), None), P(("ep", "tp"), None))
    return jax.shard_map(
        on_device, mesh=mesh, in_specs=in_specs, out_specs=out_specs, check_vma=False
    )
```

```python
import functools

import jax
import jax.numpy as jnp
from jax import lax
from jax.experimental import pallas as pl
from jax.experimental.pallas import tpu as pltpu
from jax.sharding import PartitionSpec as P

H = 32
KV = 256
ROPE = 32
NOPE = 64
V = 64
GROUPS = 4
TOPK = 2
CORES = 2
LARGE = 24


NORM_EPSILON = 1e-06
ROPE_BASE = 10000.0
F32 = jnp.float32
BF16 = jnp.bfloat16
VMEM = pl.BlockSpec(memory_space=pltpu.VMEM)
SMEM = pl.BlockSpec(memory_space=pltpu.SMEM)
HBM = pl.BlockSpec(memory_space=pltpu.HBM)


def inverse_rms(values):
    return lax.rsqrt(jnp.mean(values * values, axis=-1, keepdims=True) + NORM_EPSILON)


def iota(shape, dim):
    return lax.broadcasted_iota(jnp.int32, shape, dim)


def dot(a, b, dims=((1,), (0,)), precision=None):
    return lax.dot_general(a, b, (dims, ((), ())), precision=precision, preferred_element_type=F32)


NT = ((1,), (1,))


def attention_kernel(
    lengths_hbm,
    residual_hbm,
    query_latent_hbm,
    query_rope_hbm,
    norm_gain_hbm,
    latent_gain_hbm,
    rope_weight_hbm,
    latent_weight_hbm,
    value_weight_hbm,
    cache_latent_hbm,
    cache_rope_hbm,
    heads_out,
    new_latent_hbm,
    new_rope_hbm,
    lengths,
    new_latent_out,
    new_rope_out,
    residual,
    query_latent,
    query_rope,
    norm_gain,
    latent_gain,
    rope_weight,
    latent_weight,
    value_weight,
    cache_latent,
    cache_rope,
    mixed,
    head_rows,
    fresh_rows,
    fresh_scores,
    diagonal,
    rope_scores,
    latent_sems,
    sems,
):
    seqs = cache_latent.shape[0]
    rows = residual.shape[0]
    loads = []

    def load(source, target):
        copy = pltpu.make_async_copy(source, target, sems.at[len(loads)])
        loads.append(copy)
        copy.start()
        return copy

    rope_loads = []
    length_load = load(lengths_hbm, lengths)
    own_loads = [
        load(residual_hbm, residual),
        load(norm_gain_hbm, norm_gain),
        load(rope_weight_hbm, rope_weight),
        load(latent_gain_hbm, latent_gain),
        load(query_latent_hbm, query_latent),
        load(query_rope_hbm, query_rope),
    ]
    weight_load = load(latent_weight_hbm, latent_weight)
    for s in range(seqs):
        rope_loads.append(load(cache_rope_hbm.at[s], cache_rope.at[s]))
    for s in range(seqs):
        pltpu.make_async_copy(cache_latent_hbm.at[s], cache_latent.at[s], latent_sems.at[s]).start()
    value_load = load(value_weight_hbm, value_weight)

    lane = iota((1, ROPE), 1)
    half = ROPE // 2
    low = lane < half
    step = jnp.where(low, lane, lane - half)
    frequency = jnp.zeros((1, ROPE), F32)
    for i in range(half):
        frequency = jnp.where(step == i, F32(ROPE_BASE ** (-2.0 * i / ROPE)), frequency)
    seq_row = iota((seqs, ROPE), 0)
    length_load.wait()
    position = jnp.zeros((seqs, ROPE), F32)
    for s in range(seqs):
        position = jnp.where(seq_row == s, lengths[s].astype(F32), position)
    angles = position * frequency
    cosine = jnp.cos(angles)
    sine = jnp.sin(angles) * jnp.where(low, F32(-1), F32(1))

    for copy in own_loads:
        copy.wait()
    first = lax.axis_index("tp") * seqs
    own_pick = (iota((seqs, rows), 1) == iota((seqs, rows), 0) + first).astype(BF16)
    own = dot(own_pick, residual[...])
    normed = (own * inverse_rms(own) * norm_gain[...].astype(F32)[None, :]).astype(BF16)
    rope_rows = rope_weight[...]
    rope_swapped = jnp.concatenate([rope_rows[half:], rope_rows[:half]], axis=0)
    rope_key = dot(normed, rope_rows, NT) * cosine + dot(normed, rope_swapped, NT) * sine
    rope_key = rope_key.astype(BF16)
    new_rope_out[...] = rope_key
    rope_store = load(new_rope_out, new_rope_hbm)
    weight_load.wait()
    latent_raw = dot(normed, latent_weight[...])
    new_latent = latent_raw * inverse_rms(latent_raw) * latent_gain[...].astype(F32)[None, :]
    new_latent = new_latent.astype(BF16)
    new_latent_out[...] = new_latent
    latent_store = load(new_latent_out, new_latent_hbm)

    fresh_rows[...] = new_latent.astype(F32)

    swap = (iota((ROPE, ROPE), 0) == (iota((ROPE, ROPE), 1) + half) % ROPE).astype(BF16)
    scale = (NOPE + ROPE) ** (-0.5)
    for s in range(seqs):
        turning = query_rope[s]
        turned = turning.astype(F32) * cosine[s : s + 1] + dot(turning, swap) * sine[s : s + 1]
        turned = turned.astype(BF16).astype(F32)
        rows_of = slice(s * H, (s + 1) * H)
        fresh_scores[rows_of, :] = (
            jnp.sum(query_latent[s].astype(F32) * fresh_rows[s : s + 1, :], axis=1, keepdims=True)
            + jnp.sum(turned * rope_key[s : s + 1].astype(F32), axis=1, keepdims=True)
        ) * scale
        wide = jnp.concatenate([turned] * seqs, axis=1)
        column = iota(wide.shape, 1)
        inside = (column >= s * ROPE) & (column < (s + 1) * ROPE)
        diagonal[rows_of, :] = jnp.where(inside, wide, F32(0)).astype(BF16)
    for copy in rope_loads:
        copy.wait()
    cached = cache_latent.shape[1]
    rope_rows_all = jnp.concatenate([cache_rope[s] for s in range(seqs)], axis=0)
    rope_scores[...] = dot(diagonal[...], rope_rows_all)

    def attend(s, size):
        at = slice(s * H, (s + 1) * H)
        length = lengths[s]
        latents = cache_latent[s, :size]
        score = (dot(query_latent[s], latents, NT) + rope_scores[at, :size]) * scale
        score = jnp.where(iota(score.shape, 1) < length, score, -jnp.inf)
        fresh = fresh_scores[at, :]
        top = jnp.maximum(jnp.max(score, axis=1, keepdims=True), fresh)
        score = jnp.exp(score - top)
        fresh = jnp.exp(fresh - top)
        share = 1.0 / (jnp.sum(score, axis=1, keepdims=True) + fresh)
        mix = dot(score.astype(BF16), latents) + fresh * fresh_rows[s : s + 1, :]
        mixed[at, :] = (mix * share).astype(BF16)

    for s in range(seqs):
        pltpu.make_async_copy(cache_latent_hbm.at[s], cache_latent.at[s], latent_sems.at[s]).wait()
    for s in range(seqs):
        attend(s, cached)

    value_load.wait()
    spread = dot(mixed[...], value_weight[...])
    first = iota((H, H * V), 0) * V
    column = iota((H, H * V), 1)
    own_head = (column >= first) & (column < first + V)
    for s in range(seqs):
        kept = jnp.where(own_head, spread[s * H : (s + 1) * H], F32(0))
        head_rows[s : s + 1, :] = jnp.sum(kept, axis=0, keepdims=True)
    shares, _, width = heads_out.shape
    for t in range(shares):
        chip = t // CORES
        heads_out[t] = head_rows[:, chip * width : (chip + 1) * width].astype(BF16)
    rope_store.wait()
    latent_store.wait()


def attention(
    lengths, residual, query_latent, query_rope, norm_gain, latent_gain, rope_weight,
    latent_weight, value_weight, cache_latent, cache_rope, shares,
):
    seqs, cached, _ = cache_latent.shape
    width = H * V * CORES // shares
    in_hbm = [
        pltpu.with_memory_space_constraint(a, pltpu.HBM)
        for a in (
            lengths, residual, query_latent, query_rope, norm_gain, latent_gain, rope_weight,
            latent_weight, value_weight, cache_latent, cache_rope,
        )
    ]
    return pl.pallas_call(
        attention_kernel,
        name="attention",
        out_shape=(
            jax.ShapeDtypeStruct((shares, seqs, width), BF16),
            jax.ShapeDtypeStruct((seqs, KV), BF16),
            jax.ShapeDtypeStruct((seqs, ROPE), BF16),
        ),
        in_specs=[HBM] * 11,
        out_specs=(VMEM, HBM, HBM),
        scratch_shapes=[
            pltpu.SMEM(lengths.shape, jnp.int32),
            pltpu.VMEM((seqs, KV), BF16),
            pltpu.VMEM((seqs, ROPE), BF16),
            pltpu.VMEM(residual.shape, BF16),
            pltpu.VMEM(query_latent.shape, BF16),
            pltpu.VMEM(query_rope.shape, BF16),
            pltpu.VMEM(norm_gain.shape, BF16),
            pltpu.VMEM(latent_gain.shape, BF16),
            pltpu.VMEM(rope_weight.shape, BF16),
            pltpu.VMEM(latent_weight.shape, BF16),
            pltpu.VMEM(value_weight.shape, BF16),
            pltpu.VMEM(cache_latent.shape, BF16),
            pltpu.VMEM(cache_rope.shape, BF16),
            pltpu.VMEM((seqs * H, KV), BF16),
            pltpu.VMEM((seqs, H * V), F32),
            pltpu.VMEM((seqs, KV), F32),
            pltpu.VMEM((seqs * H, 1), F32),
            pltpu.VMEM((seqs * H, seqs * ROPE), BF16),
            pltpu.VMEM((seqs * H, cached), F32),
            pltpu.SemaphoreType.DMA((seqs,)),
            pltpu.SemaphoreType.DMA((seqs + 11,)),
        ],
        compiler_params=pltpu.CompilerParams(vmem_limit_bytes=LARGE * 2**20),
        cost_estimate=pl.CostEstimate(
            flops=2 * seqs * H * cached * (2 * KV + ROPE), bytes_accessed=8 * 2**20, transcendentals=0
        ),
    )(*in_hbm)


def own_half(width):
    core = lax.rem(lax.axis_index("tp"), CORES)
    return pl.multiple_of(core * width, width), pl.multiple_of((1 - core) * width, width)


def tree_sum(terms):
    while len(terms) > 1:
        terms = [terms[i] + terms[i + 1] for i in range(0, len(terms), 2)]
    return terms[0]


def call(kernel, name, out_shape, scratch, operands, **params):
    limit = params.pop("limit", 8)
    flops = params.pop("flops", 10**6)
    moved = params.pop("moved", 2**20)
    return pl.pallas_call(
        kernel,
        name=name,
        out_shape=out_shape,
        scratch_shapes=scratch,
        compiler_params=pltpu.CompilerParams(vmem_limit_bytes=limit * 2**20),
        cost_estimate=pl.CostEstimate(flops=flops, bytes_accessed=moved, transcendentals=0),
        **params,
    )(*operands)


def shaped(shape, dtype=BF16):
    return jax.ShapeDtypeStruct(shape, dtype)


def project_kernel(heads, own_weight, other_weight, terms_out, gathered):
    shares, seqs, _ = heads.shape
    for t in range(shares):
        gathered[t * seqs : (t + 1) * seqs, :] = heads[t].astype(F32)
    own_rows, other_rows = own_half(own_weight.shape[0])
    width = terms_out.shape[1]
    columns = pl.ds(own_half(width)[0], width)
    terms = dot(
        gathered[:, pl.ds(own_rows, own_weight.shape[0])].astype(BF16), own_weight[:, columns]
    ) + dot(
        gathered[:, pl.ds(other_rows, own_weight.shape[0])].astype(BF16), other_weight[:, columns]
    )
    terms_out[...] = terms.astype(BF16)


def project(heads, own_weight, other_weight):
    shares, seqs, width = heads.shape
    columns = own_weight.shape[1] // CORES
    return call(
        project_kernel, "project", shaped((shares * seqs, columns)),
        [pltpu.VMEM((shares * seqs, width), F32)], (heads, own_weight, other_weight),
        in_specs=[VMEM] * 3, out_specs=VMEM, flops=10**10, moved=2**25,
    )


def dispatch_kernel(count, local_experts, slots, *refs):
    terms, (residual, expert_ids), outs = refs[:count], refs[count : count + 2], refs[count + 2 :]
    sent_out, (after_out, pick_out) = outs[:-2], outs[-2:]
    rows, width = terms[0].shape
    total = tree_sum([part[...].astype(F32) for part in terms])
    own_columns = pl.ds(own_half(width)[0], width)
    after = (residual[:, own_columns].astype(F32) + total).astype(BF16)
    after_out[...] = after

    ep_count = len(sent_out)
    index = (iota((ep_count, rows), 0) ^ lax.axis_index("ep")) * local_experts
    hit = None
    for k in range(TOPK):
        named = expert_ids[k : k + 1, :]
        here = (named >= index) & (named < index + local_experts)
        hit = here if hit is None else hit | here
    hit = hit.astype(F32)
    earlier = (iota((rows, rows), 0) < iota((rows, rows), 1)).astype(BF16)
    rank = jnp.where(hit > 0.5, dot(hit.astype(BF16), earlier), F32(-1))
    slot = iota((slots, rows), 0).astype(F32)
    pick = jnp.concatenate(
        [(rank[e : e + 1, :] == slot).astype(F32) for e in range(ep_count)], axis=0
    ).astype(BF16)
    pick_out[...] = pick
    chosen = dot(pick, after).astype(BF16)
    for e in range(ep_count):
        sent_out[e][...] = chosen[e * slots : (e + 1) * slots]


def dispatch(terms, residual, expert_ids, ep_count, local_experts, slots):
    rows, width = terms[0].shape
    outs = call(
        functools.partial(dispatch_kernel, len(terms), local_experts, slots), "dispatch",
        (shaped((slots, width)),) * ep_count
        + (shaped((rows, width)), shaped((ep_count * slots, rows))),
        [], (*terms, residual, expert_ids),
        in_specs=[VMEM] * (len(terms) + 2), out_specs=(VMEM,) * (ep_count + 2),
    )
    return outs[:ep_count], outs[ep_count], outs[ep_count + 1]


def experts_kernel(
    own_rows, other_rows, mixer_gain, group_router, expert_router, *refs
):
    *choice, gate, up, down, keep_out, give_out, rows_in = refs
    width = own_rows.shape[1]
    own_at, other_at = own_half(width)
    rows_in[:, pl.ds(own_at, width)] = own_rows[...].astype(F32)
    rows_in[:, pl.ds(other_at, width)] = other_rows[...].astype(F32)
    after = rows_in[...]
    expert_in = (after * inverse_rms(after) * mixer_gain[...].astype(F32)[None, :]).astype(BF16)

    group_logits = dot(expert_in, group_router[...], NT)
    expert_logits = dot(expert_in, expert_router[...], NT)
    first = lax.axis_index("ep") * gate.shape[0]
    if choice:
        chosen = choice[0][...]
        ids, group = [chosen[:, k : k + 1] for k in range(TOPK)], chosen[:, TOPK : TOPK + 1]
    else:
        ids, group = [first + k for k in range(TOPK)], lax.axis_index("ep")
    group_hit = iota(group_logits.shape, 1) == group
    own_group = jnp.sum(jnp.where(group_hit, group_logits, F32(0)), axis=1, keepdims=True)
    group_share = 1.0 / jnp.sum(jnp.exp(group_logits - own_group), axis=1, keepdims=True)
    picked = []
    for k in range(TOPK):
        expert_hit = iota(expert_logits.shape, 1) == ids[k]
        picked.append(jnp.sum(jnp.where(expert_hit, expert_logits, F32(0)), axis=1, keepdims=True))
    route = []
    for k in range(TOPK):
        total = jnp.exp(picked[0] - picked[k])
        for j in range(1, TOPK):
            total = total + jnp.exp(picked[j] - picked[k])
        route.append(group_share / total)

    result = None
    for l in range(gate.shape[0]):
        weight = jnp.where(ids[0] == first + l, route[0], F32(0))
        for k in range(1, TOPK):
            weight = weight + jnp.where(ids[k] == first + l, route[k], F32(0))
        gated = dot(expert_in, gate[l])
        raised = dot(expert_in, up[l])
        act = (gated / (1.0 + jnp.exp(-gated)) * raised).astype(BF16)
        part = dot(act, down[l]) * weight
        result = part if result is None else result + part
    rows_in[...] = result
    keep_out[...] = rows_in[:, pl.ds(own_at, width)]
    give_out[...] = rows_in[:, pl.ds(other_at, width)].astype(BF16)


def run_experts(own_rows, other_rows, mixer_gain, group_router, expert_router, choice, weights):
    rows, width = own_rows.shape
    gate, up, down = weights
    gate = pltpu.with_memory_space_constraint(gate, pltpu.VMEM)
    up = pltpu.with_memory_space_constraint(up, pltpu.VMEM)
    down = pltpu.with_memory_space_constraint(down, pltpu.VMEM)
    return call(
        experts_kernel, "experts",
        (shaped((rows, width), F32), shaped((rows, width))),
        [
            pltpu.VMEM((rows, CORES * width), F32),
        ],
        (own_rows, other_rows, mixer_gain, group_router, expert_router, *choice, gate, up, down),
        in_specs=[VMEM] * (8 + len(choice)), out_specs=(VMEM, VMEM),
        flops=6 * rows * gate.size, moved=6 * gate.size, limit=LARGE,
    )


def fold_kernel(keep, came, *blocks_out):
    total = (keep[...] + came[...].astype(F32)).astype(BF16)
    slots = blocks_out[0].shape[0]
    for e, block in enumerate(blocks_out):
        block[...] = total[e * slots : (e + 1) * slots]


def fold(keep, came, ep_count):
    rows, width = keep.shape
    return call(
        fold_kernel, "fold", (shaped((rows // ep_count, width)),) * ep_count, [], (keep, came),
        in_specs=[VMEM] * 2, out_specs=(VMEM,) * ep_count,
    )


def collect_kernel(pick, *refs):
    *blocks, out = refs
    back = jnp.concatenate([block[...] for block in blocks], axis=0)
    out[...] = dot(pick[...], back, ((0,), (0,))).astype(BF16)


def collect(pick, blocks):
    return call(
        collect_kernel, "collect", shaped((pick.shape[1], blocks[0].shape[1])), [],
        (pick, *blocks), in_specs=[VMEM] * (1 + len(blocks)), out_specs=VMEM,
    )


def mix_kernel(after, *refs):
    *terms, out = refs
    total = tree_sum([part[...].astype(F32) for part in terms])
    out[...] = (after[...].astype(F32) + total).astype(BF16)


def mix(after, terms):
    return call(
        mix_kernel, "mix", shaped(after.shape), [], (after, *terms),
        in_specs=[VMEM] * (1 + len(terms)), out_specs=VMEM,
    )


def place_kernel(own, other, out):
    width = own.shape[1]
    own_at, other_at = own_half(width)
    out[:, pl.ds(own_at, width)] = own[...]
    out[:, pl.ds(other_at, width)] = other[...]


def place_halves(own, other):
    rows, width = own.shape
    return call(
        place_kernel, "place", shaped((rows, CORES * width)), [], (own, other),
        in_specs=[VMEM] * 2, out_specs=VMEM,
    )


def flip(block, axis, bits):
    return lax.ppermute(block, axis, [(i, i ^ bits) for i in range(lax.axis_size(axis))])


def from_chips(block):
    chips = lax.axis_size("tp") // CORES
    return [block] + [flip(block, "tp", CORES * m) for m in range(1, chips)]


def swap_blocks(blocks):
    return [blocks[0]] + [flip(blocks[m], "ep", m) for m in range(1, len(blocks))]


def exchange(blocks, axis):
    return lax.all_to_all(blocks, axis, split_axis=0, concat_axis=0, tiled=True)


def slot_owners(expert_ids, local_experts):
    return (expert_ids // local_experts).T


def slot_table(owners, index, slots):
    hit = jnp.any(owners == index, axis=0).astype(jnp.int32)
    rank = jnp.cumsum(hit) - hit
    return (rank[None, :] == jnp.arange(slots)[:, None]) & (hit[None, :] > 0)


def on_device(
    residual,
    cache_latent,
    cache_rope,
    lengths,
    query_latent,
    query_rope,
    norm_gain,
    latent_weight,
    latent_gain,
    rope_weight,
    value_weight,
    out_weight,
    mixer_gain,
    group_router,
    expert_router,
    expert_ids,
    gate_weight,
    up_weight,
    down_weight,
):
    ep_count = lax.axis_size("ep")
    tp_count = lax.axis_size("tp")
    group_rows, model_width = residual.shape
    experts = expert_router.shape[1]
    per_group = experts // GROUPS
    local_experts = gate_weight.shape[0]
    capacity = 2 * group_rows * TOPK // experts
    whole_groups = per_group == TOPK and local_experts == TOPK
    slots = capacity if whole_groups else capacity * local_experts
    choice = ()
    if not whole_groups:
        here = lax.axis_index("ep")
        order = here ^ jnp.arange(ep_count, dtype=jnp.int32)
        all_ids = jnp.take(lax.all_gather(expert_ids, "ep"), order, axis=0)
        mine = jax.vmap(lambda ids: slot_table(slot_owners(ids, local_experts), here, slots))(all_ids)
        slot_ids = jnp.sum(
            mine[:, :, :, None].astype(jnp.int32) * all_ids[:, None, :, :], axis=2
        ).reshape(-1, TOPK)
        choice = (jnp.concatenate([slot_ids, slot_ids[:, :1] // per_group], axis=1),)

    other_weight = flip(out_weight, "tp", 1)
    heads, new_latent, new_rope_key = attention(
        lengths, residual, query_latent, query_rope, norm_gain, latent_gain,
        rope_weight, latent_weight, value_weight, cache_latent, cache_rope, tp_count,
    )
    terms = project(exchange(heads, "tp"), out_weight, other_weight)
    sent, after, pick = dispatch(
        from_chips(terms), residual, expert_ids.T, ep_count, local_experts, slots
    )
    own_rows = jnp.concatenate(swap_blocks(sent), axis=0)
    keep, give = run_experts(
        own_rows, flip(own_rows, "tp", 1), mixer_gain, group_router.T, expert_router.T, choice,
        (gate_weight, up_weight, down_weight),
    )
    back = swap_blocks(fold(keep, flip(give, "tp", 1), ep_count))
    mixed_half = mix(after, from_chips(collect(pick, back)))
    mixed = place_halves(mixed_half, flip(mixed_half, "tp", 1))
    return (mixed, new_latent, new_rope_key)


def solution(mesh):
    in_specs = (
        P("ep", None),
        P(("ep", "tp"), None, None),
        P(("ep", "tp"), None, None),
        P(("ep", "tp")),
        P(("ep", "tp"), None, None),
        P(("ep", "tp"), None, None),
        P(),
        P(),
        P(),
        P(),
        P(),
        P("tp", None),
        P(),
        P(),
        P(),
        P("ep", None),
        P("ep", None, "tp"),
        P("ep", None, "tp"),
        P("ep", "tp", None),
    )
    out_specs = (P("ep", None), P(("ep", "tp"), None), P(("ep", "tp"), None))
    return jax.shard_map(
        on_device, mesh=mesh, in_specs=in_specs, out_specs=out_specs, check_vma=False
    )
```

```python
import functools

import jax
import jax.numpy as jnp
from jax import lax
from jax.experimental import pallas as pl
from jax.experimental.pallas import tpu as pltpu
from jax.sharding import PartitionSpec as P

H = 32
KV = 256
ROPE = 32
NOPE = 64
V = 64
GROUPS = 4
TOPK = 2
CORES = 2
LANES = 128
LARGE = 24


NORM_EPSILON = 1e-06
ROPE_BASE = 10000.0
F32 = jnp.float32
BF16 = jnp.bfloat16
VMEM = pl.BlockSpec(memory_space=pltpu.VMEM)
SMEM = pl.BlockSpec(memory_space=pltpu.SMEM)
HBM = pl.BlockSpec(memory_space=pltpu.HBM)


def inverse_rms(values):
    return lax.rsqrt(jnp.mean(values * values, axis=-1, keepdims=True) + NORM_EPSILON)


def iota(shape, dim):
    return lax.broadcasted_iota(jnp.int32, shape, dim)


def dot(a, b, dims=((1,), (0,)), precision=None):
    return lax.dot_general(a, b, (dims, ((), ())), precision=precision, preferred_element_type=F32)


NT = ((1,), (1,))


def attention_kernel(
    lengths_hbm,
    residual_hbm,
    query_latent_hbm,
    query_rope_hbm,
    norm_gain_hbm,
    latent_gain_hbm,
    rope_weight_hbm,
    latent_weight_hbm,
    value_weight_hbm,
    cache_latent_hbm,
    cache_rope_hbm,
    heads_out,
    new_latent_hbm,
    new_rope_hbm,
    lengths,
    new_latent_out,
    new_rope_out,
    residual,
    query_latent,
    query_rope,
    norm_gain,
    latent_gain,
    rope_weight,
    latent_weight,
    value_weight,
    cache_latent,
    cache_rope,
    mixed,
    head_rows,
    fresh_rows,
    fresh_scores,
    diagonal,
    rope_scores,
    latent_sems,
    sems,
):
    seqs = cache_latent.shape[0]
    rows = residual.shape[0]
    loads = []

    def load(source, target):
        copy = pltpu.make_async_copy(source, target, sems.at[len(loads)])
        loads.append(copy)
        copy.start()
        return copy

    rope_loads = []
    length_load = load(lengths_hbm, lengths)
    own_loads = [
        load(residual_hbm, residual),
        load(norm_gain_hbm, norm_gain),
        load(rope_weight_hbm, rope_weight),
        load(latent_gain_hbm, latent_gain),
        load(query_latent_hbm, query_latent),
        load(query_rope_hbm, query_rope),
    ]
    weight_load = load(latent_weight_hbm, latent_weight)
    for s in range(seqs):
        rope_loads.append(load(cache_rope_hbm.at[s], cache_rope.at[s]))
    for s in range(seqs):
        pltpu.make_async_copy(cache_latent_hbm.at[s], cache_latent.at[s], latent_sems.at[s]).start()
    value_load = load(value_weight_hbm, value_weight)

    lane = iota((1, ROPE), 1)
    half = ROPE // 2
    low = lane < half
    step = jnp.where(low, lane, lane - half)
    frequency = jnp.zeros((1, ROPE), F32)
    for i in range(half):
        frequency = jnp.where(step == i, F32(ROPE_BASE ** (-2.0 * i / ROPE)), frequency)
    seq_row = iota((seqs, ROPE), 0)
    length_load.wait()
    position = jnp.zeros((seqs, ROPE), F32)
    for s in range(seqs):
        position = jnp.where(seq_row == s, lengths[s].astype(F32), position)
    angles = position * frequency
    cosine = jnp.cos(angles)
    sine = jnp.sin(angles) * jnp.where(low, F32(-1), F32(1))

    for copy in own_loads:
        copy.wait()
    first = lax.axis_index("tp") * seqs
    own_pick = (iota((seqs, rows), 1) == iota((seqs, rows), 0) + first).astype(BF16)
    own = dot(own_pick, residual[...])
    normed = (own * inverse_rms(own) * norm_gain[...].astype(F32)[None, :]).astype(BF16)
    rope_rows = rope_weight[...]
    rope_swapped = jnp.concatenate([rope_rows[half:], rope_rows[:half]], axis=0)
    rope_key = dot(normed, rope_rows, NT) * cosine + dot(normed, rope_swapped, NT) * sine
    rope_key = rope_key.astype(BF16)
    new_rope_out[...] = rope_key
    rope_store = load(new_rope_out, new_rope_hbm)
    weight_load.wait()
    latent_raw = dot(normed, latent_weight[...])
    new_latent = latent_raw * inverse_rms(latent_raw) * latent_gain[...].astype(F32)[None, :]
    new_latent = new_latent.astype(BF16)
    new_latent_out[...] = new_latent
    latent_store = load(new_latent_out, new_latent_hbm)

    fresh_rows[...] = new_latent.astype(F32)

    swap = (iota((ROPE, ROPE), 0) == (iota((ROPE, ROPE), 1) + half) % ROPE).astype(BF16)
    scale = (NOPE + ROPE) ** (-0.5)
    for s in range(seqs):
        turning = query_rope[s]
        turned = turning.astype(F32) * cosine[s : s + 1] + dot(turning, swap) * sine[s : s + 1]
        turned = turned.astype(BF16).astype(F32)
        rows_of = slice(s * H, (s + 1) * H)
        fresh_scores[rows_of, :] = (
            jnp.sum(query_latent[s].astype(F32) * fresh_rows[s : s + 1, :], axis=1, keepdims=True)
            + jnp.sum(turned * rope_key[s : s + 1].astype(F32), axis=1, keepdims=True)
        ) * scale
        wide = jnp.concatenate([turned] * seqs, axis=1)
        column = iota(wide.shape, 1)
        inside = (column >= s * ROPE) & (column < (s + 1) * ROPE)
        diagonal[rows_of, :] = jnp.where(inside, wide, F32(0)).astype(BF16)
    for copy in rope_loads:
        copy.wait()
    cached = cache_latent.shape[1]
    rope_rows_all = jnp.concatenate([cache_rope[s] for s in range(seqs)], axis=0)
    rope_scores[...] = dot(diagonal[...], rope_rows_all)

    def attend(s, size):
        at = pl.ds(pl.multiple_of(s * H, H), H)
        length = lengths[s]
        latents = cache_latent[s, :size]
        score = (dot(query_latent[s], latents, NT) + rope_scores[at, :size]) * scale
        score = jnp.where(iota(score.shape, 1) < length, score, -jnp.inf)
        fresh = fresh_scores[at, :]
        top = jnp.maximum(jnp.max(score, axis=1, keepdims=True), fresh)
        score = jnp.exp(score - top)
        fresh = jnp.exp(fresh - top)
        share = 1.0 / (jnp.sum(score, axis=1, keepdims=True) + fresh)
        mix = dot(score.astype(BF16), latents) + fresh * fresh_rows[pl.ds(s, 1), :]
        mix = mix * share
        for n in range(KV // LANES):
            mixed[n, pl.ds(s, H, seqs), :] = mix[:, n * LANES : (n + 1) * LANES]

    sizes = (cached // 8, cached // 4, cached // 2, cached * 3 // 4, cached)

    def one(s, carry):
        pltpu.make_async_copy(cache_latent_hbm.at[s], cache_latent.at[s], latent_sems.at[s]).wait()
        below = 0
        for size in sizes:
            here = lengths[s] > below
            if size < cached:
                here = here & (lengths[s] <= size)
            pl.when(here)(functools.partial(attend, s, size))
            below = size
        return carry

    lax.fori_loop(0, seqs, one, 0)

    value_load.wait()
    heads = 256 // V
    tile = heads * V
    own_seqs = iota((seqs, tile), 1)
    for j in range(H // heads):
        rows_of = slice(j * heads * seqs, (j + 1) * heads * seqs)
        taken = jnp.concatenate([mixed[n, rows_of, :] for n in range(KV // LANES)], axis=1)
        spread = dot(taken.astype(BF16), value_weight[:, j * tile : (j + 1) * tile])
        kept = spread[:seqs]
        for h in range(1, heads):
            kept = jnp.where(own_seqs >= h * V, spread[h * seqs : (h + 1) * seqs], kept)
        head_rows[:, j * tile : (j + 1) * tile] = kept
    shares, _, width = heads_out.shape
    for t in range(shares):
        chip = t // CORES
        heads_out[t] = head_rows[:, chip * width : (chip + 1) * width].astype(BF16)
    rope_store.wait()
    latent_store.wait()


def attention(
    lengths, residual, query_latent, query_rope, norm_gain, latent_gain, rope_weight,
    latent_weight, value_weight, cache_latent, cache_rope, shares,
):
    seqs, cached, _ = cache_latent.shape
    width = H * V * CORES // shares
    in_hbm = [
        pltpu.with_memory_space_constraint(a, pltpu.HBM)
        for a in (
            lengths, residual, query_latent, query_rope, norm_gain, latent_gain, rope_weight,
            latent_weight, value_weight, cache_latent, cache_rope,
        )
    ]
    return pl.pallas_call(
        attention_kernel,
        name="attention",
        out_shape=(
            jax.ShapeDtypeStruct((shares, seqs, width), BF16),
            jax.ShapeDtypeStruct((seqs, KV), BF16),
            jax.ShapeDtypeStruct((seqs, ROPE), BF16),
        ),
        in_specs=[HBM] * 11,
        out_specs=(VMEM, HBM, HBM),
        scratch_shapes=[
            pltpu.SMEM(lengths.shape, jnp.int32),
            pltpu.VMEM((seqs, KV), BF16),
            pltpu.VMEM((seqs, ROPE), BF16),
            pltpu.VMEM(residual.shape, BF16),
            pltpu.VMEM(query_latent.shape, BF16),
            pltpu.VMEM(query_rope.shape, BF16),
            pltpu.VMEM(norm_gain.shape, BF16),
            pltpu.VMEM(latent_gain.shape, BF16),
            pltpu.VMEM(rope_weight.shape, BF16),
            pltpu.VMEM(latent_weight.shape, BF16),
            pltpu.VMEM(value_weight.shape, BF16),
            pltpu.VMEM(cache_latent.shape, BF16),
            pltpu.VMEM(cache_rope.shape, BF16),
            pltpu.VMEM((KV // LANES, seqs * H, LANES), F32),
            pltpu.VMEM((seqs, H * V), F32),
            pltpu.VMEM((seqs, KV), F32),
            pltpu.VMEM((seqs * H, 1), F32),
            pltpu.VMEM((seqs * H, seqs * ROPE), BF16),
            pltpu.VMEM((seqs * H, cached), F32),
            pltpu.SemaphoreType.DMA((seqs,)),
            pltpu.SemaphoreType.DMA((seqs + 11,)),
        ],
        compiler_params=pltpu.CompilerParams(vmem_limit_bytes=LARGE * 2**20),
        cost_estimate=pl.CostEstimate(
            flops=2 * seqs * H * cached * (2 * KV + ROPE), bytes_accessed=8 * 2**20, transcendentals=0
        ),
    )(*in_hbm)


def own_half(width):
    core = lax.rem(lax.axis_index("tp"), CORES)
    return pl.multiple_of(core * width, width), pl.multiple_of((1 - core) * width, width)


def tree_sum(terms):
    while len(terms) > 1:
        terms = [terms[i] + terms[i + 1] for i in range(0, len(terms), 2)]
    return terms[0]


def call(kernel, name, out_shape, scratch, operands, **params):
    limit = params.pop("limit", 8)
    flops = params.pop("flops", 10**6)
    moved = params.pop("moved", 2**20)
    return pl.pallas_call(
        kernel,
        name=name,
        out_shape=out_shape,
        scratch_shapes=scratch,
        compiler_params=pltpu.CompilerParams(vmem_limit_bytes=limit * 2**20),
        cost_estimate=pl.CostEstimate(flops=flops, bytes_accessed=moved, transcendentals=0),
        **params,
    )(*operands)


def shaped(shape, dtype=BF16):
    return jax.ShapeDtypeStruct(shape, dtype)


def project_kernel(heads, own_weight, other_weight, terms_out, gathered):
    shares, seqs, _ = heads.shape
    for t in range(shares):
        gathered[t * seqs : (t + 1) * seqs, :] = heads[t].astype(F32)
    own_rows, other_rows = own_half(own_weight.shape[0])
    width = terms_out.shape[1]
    columns = pl.ds(own_half(width)[0], width)
    terms = dot(
        gathered[:, pl.ds(own_rows, own_weight.shape[0])].astype(BF16), own_weight[:, columns]
    ) + dot(
        gathered[:, pl.ds(other_rows, own_weight.shape[0])].astype(BF16), other_weight[:, columns]
    )
    terms_out[...] = terms.astype(BF16)


def project(heads, own_weight, other_weight):
    shares, seqs, width = heads.shape
    columns = own_weight.shape[1] // CORES
    return call(
        project_kernel, "project", shaped((shares * seqs, columns)),
        [pltpu.VMEM((shares * seqs, width), F32)], (heads, own_weight, other_weight),
        in_specs=[VMEM] * 3, out_specs=VMEM, flops=10**10, moved=2**25,
    )


def dispatch_kernel(count, local_experts, slots, *refs):
    terms, (residual, expert_ids), outs = refs[:count], refs[count : count + 2], refs[count + 2 :]
    sent_out, (after_out, pick_out) = outs[:-2], outs[-2:]
    rows, width = terms[0].shape
    total = tree_sum([part[...].astype(F32) for part in terms])
    own_columns = pl.ds(own_half(width)[0], width)
    after = (residual[:, own_columns].astype(F32) + total).astype(BF16)
    after_out[...] = after

    ep_count = len(sent_out)
    index = (iota((ep_count, rows), 0) ^ lax.axis_index("ep")) * local_experts
    hit = None
    for k in range(TOPK):
        named = expert_ids[k : k + 1, :]
        here = (named >= index) & (named < index + local_experts)
        hit = here if hit is None else hit | here
    hit = hit.astype(F32)
    earlier = (iota((rows, rows), 0) < iota((rows, rows), 1)).astype(BF16)
    rank = jnp.where(hit > 0.5, dot(hit.astype(BF16), earlier), F32(-1))
    slot = iota((slots, rows), 0).astype(F32)
    pick = jnp.concatenate(
        [(rank[e : e + 1, :] == slot).astype(F32) for e in range(ep_count)], axis=0
    ).astype(BF16)
    pick_out[...] = pick
    chosen = dot(pick, after).astype(BF16)
    for e in range(ep_count):
        sent_out[e][...] = chosen[e * slots : (e + 1) * slots]


def dispatch(terms, residual, expert_ids, ep_count, local_experts, slots):
    rows, width = terms[0].shape
    outs = call(
        functools.partial(dispatch_kernel, len(terms), local_experts, slots), "dispatch",
        (shaped((slots, width)),) * ep_count
        + (shaped((rows, width)), shaped((ep_count * slots, rows))),
        [], (*terms, residual, expert_ids),
        in_specs=[VMEM] * (len(terms) + 2), out_specs=(VMEM,) * (ep_count + 2),
    )
    return outs[:ep_count], outs[ep_count], outs[ep_count + 1]


def experts_kernel(
    own_rows, other_rows, mixer_gain, group_router, expert_router, *refs
):
    *choice, gate, up, down, keep_out, give_out, rows_in = refs
    width = own_rows.shape[1]
    own_at, other_at = own_half(width)
    rows_in[:, pl.ds(own_at, width)] = own_rows[...].astype(F32)
    rows_in[:, pl.ds(other_at, width)] = other_rows[...].astype(F32)
    after = rows_in[...]
    expert_in = (after * inverse_rms(after) * mixer_gain[...].astype(F32)[None, :]).astype(BF16)

    group_logits = dot(expert_in, group_router[...], NT)
    expert_logits = dot(expert_in, expert_router[...], NT)
    first = lax.axis_index("ep") * gate.shape[0]
    if choice:
        chosen = choice[0][...]
        ids, group = [chosen[:, k : k + 1] for k in range(TOPK)], chosen[:, TOPK : TOPK + 1]
    else:
        ids, group = [first + k for k in range(TOPK)], lax.axis_index("ep")
    group_hit = iota(group_logits.shape, 1) == group
    own_group = jnp.sum(jnp.where(group_hit, group_logits, F32(0)), axis=1, keepdims=True)
    group_share = 1.0 / jnp.sum(jnp.exp(group_logits - own_group), axis=1, keepdims=True)
    picked = []
    for k in range(TOPK):
        expert_hit = iota(expert_logits.shape, 1) == ids[k]
        picked.append(jnp.sum(jnp.where(expert_hit, expert_logits, F32(0)), axis=1, keepdims=True))
    route = []
    for k in range(TOPK):
        total = jnp.exp(picked[0] - picked[k])
        for j in range(1, TOPK):
            total = total + jnp.exp(picked[j] - picked[k])
        route.append(group_share / total)

    result = None
    for l in range(gate.shape[0]):
        weight = jnp.where(ids[0] == first + l, route[0], F32(0))
        for k in range(1, TOPK):
            weight = weight + jnp.where(ids[k] == first + l, route[k], F32(0))
        gated = dot(expert_in, gate[l])
        raised = dot(expert_in, up[l])
        act = (gated / (1.0 + jnp.exp(-gated)) * raised).astype(BF16)
        part = dot(act, down[l]) * weight
        result = part if result is None else result + part
    rows_in[...] = result
    keep_out[...] = rows_in[:, pl.ds(own_at, width)]
    give_out[...] = rows_in[:, pl.ds(other_at, width)].astype(BF16)


def run_experts(own_rows, other_rows, mixer_gain, group_router, expert_router, choice, weights):
    rows, width = own_rows.shape
    gate, up, down = weights
    gate = pltpu.with_memory_space_constraint(gate, pltpu.VMEM)
    up = pltpu.with_memory_space_constraint(up, pltpu.VMEM)
    down = pltpu.with_memory_space_constraint(down, pltpu.VMEM)
    return call(
        experts_kernel, "experts",
        (shaped((rows, width), F32), shaped((rows, width))),
        [
            pltpu.VMEM((rows, CORES * width), F32),
        ],
        (own_rows, other_rows, mixer_gain, group_router, expert_router, *choice, gate, up, down),
        in_specs=[VMEM] * (8 + len(choice)), out_specs=(VMEM, VMEM),
        flops=6 * rows * gate.size, moved=6 * gate.size, limit=LARGE,
    )


def fold_kernel(keep, came, *blocks_out):
    total = (keep[...] + came[...].astype(F32)).astype(BF16)
    slots = blocks_out[0].shape[0]
    for e, block in enumerate(blocks_out):
        block[...] = total[e * slots : (e + 1) * slots]


def fold(keep, came, ep_count):
    rows, width = keep.shape
    return call(
        fold_kernel, "fold", (shaped((rows // ep_count, width)),) * ep_count, [], (keep, came),
        in_specs=[VMEM] * 2, out_specs=(VMEM,) * ep_count,
    )


def collect_kernel(pick, *refs):
    *blocks, out = refs
    back = jnp.concatenate([block[...] for block in blocks], axis=0)
    out[...] = dot(pick[...], back, ((0,), (0,))).astype(BF16)


def collect(pick, blocks):
    return call(
        collect_kernel, "collect", shaped((pick.shape[1], blocks[0].shape[1])), [],
        (pick, *blocks), in_specs=[VMEM] * (1 + len(blocks)), out_specs=VMEM,
    )


def mix_kernel(after, *refs):
    *terms, out = refs
    total = tree_sum([part[...].astype(F32) for part in terms])
    out[...] = (after[...].astype(F32) + total).astype(BF16)


def mix(after, terms):
    return call(
        mix_kernel, "mix", shaped(after.shape), [], (after, *terms),
        in_specs=[VMEM] * (1 + len(terms)), out_specs=VMEM,
    )


def place_kernel(own, other, out, sems):
    width = own.shape[1]
    own_at, other_at = own_half(width)
    copies = [
        pltpu.make_async_copy(own, out.at[:, pl.ds(own_at, width)], sems.at[0]),
        pltpu.make_async_copy(other, out.at[:, pl.ds(other_at, width)], sems.at[1]),
    ]
    for copy in copies:
        copy.start()
    for copy in copies:
        copy.wait()


def place_halves(own, other):
    rows, width = own.shape
    return call(
        place_kernel, "place", shaped((rows, CORES * width)), [pltpu.SemaphoreType.DMA((2,))],
        (own, other), in_specs=[VMEM] * 2, out_specs=HBM,
    )


def flip(block, axis, bits):
    return lax.ppermute(block, axis, [(i, i ^ bits) for i in range(lax.axis_size(axis))])


def from_chips(block):
    chips = lax.axis_size("tp") // CORES
    return [block] + [flip(block, "tp", CORES * m) for m in range(1, chips)]


def swap_blocks(blocks):
    return [blocks[0]] + [flip(blocks[m], "ep", m) for m in range(1, len(blocks))]


def exchange(blocks, axis):
    return lax.all_to_all(blocks, axis, split_axis=0, concat_axis=0, tiled=True)


def slot_owners(expert_ids, local_experts):
    return (expert_ids // local_experts).T


def slot_table(owners, index, slots):
    hit = jnp.any(owners == index, axis=0).astype(jnp.int32)
    rank = jnp.cumsum(hit) - hit
    return (rank[None, :] == jnp.arange(slots)[:, None]) & (hit[None, :] > 0)


def on_device(
    residual,
    cache_latent,
    cache_rope,
    lengths,
    query_latent,
    query_rope,
    norm_gain,
    latent_weight,
    latent_gain,
    rope_weight,
    value_weight,
    out_weight,
    mixer_gain,
    group_router,
    expert_router,
    expert_ids,
    gate_weight,
    up_weight,
    down_weight,
):
    ep_count = lax.axis_size("ep")
    tp_count = lax.axis_size("tp")
    group_rows, model_width = residual.shape
    experts = expert_router.shape[1]
    per_group = experts // GROUPS
    local_experts = gate_weight.shape[0]
    capacity = 2 * group_rows * TOPK // experts
    whole_groups = per_group == TOPK and local_experts == TOPK
    slots = capacity if whole_groups else capacity * local_experts
    choice = ()
    if not whole_groups:
        here = lax.axis_index("ep")
        order = here ^ jnp.arange(ep_count, dtype=jnp.int32)
        all_ids = jnp.take(lax.all_gather(expert_ids, "ep"), order, axis=0)
        mine = jax.vmap(lambda ids: slot_table(slot_owners(ids, local_experts), here, slots))(all_ids)
        slot_ids = jnp.sum(
            mine[:, :, :, None].astype(jnp.int32) * all_ids[:, None, :, :], axis=2
        ).reshape(-1, TOPK)
        choice = (jnp.concatenate([slot_ids, slot_ids[:, :1] // per_group], axis=1),)

    other_weight = flip(out_weight, "tp", 1)
    heads, new_latent, new_rope_key = attention(
        lengths, residual, query_latent, query_rope, norm_gain, latent_gain,
        rope_weight, latent_weight, value_weight, cache_latent, cache_rope, tp_count,
    )
    terms = project(exchange(heads, "tp"), out_weight, other_weight)
    sent, after, pick = dispatch(
        from_chips(terms), residual, expert_ids.T, ep_count, local_experts, slots
    )
    own_rows = jnp.concatenate(swap_blocks(sent), axis=0)
    keep, give = run_experts(
        own_rows, flip(own_rows, "tp", 1), mixer_gain, group_router.T, expert_router.T, choice,
        (gate_weight, up_weight, down_weight),
    )
    back = swap_blocks(fold(keep, flip(give, "tp", 1), ep_count))
    mixed_half = mix(after, from_chips(collect(pick, back)))
    mixed = place_halves(mixed_half, flip(mixed_half, "tp", 1))
    return (mixed, new_latent, new_rope_key)


def solution(mesh):
    in_specs = (
        P("ep", None),
        P(("ep", "tp"), None, None),
        P(("ep", "tp"), None, None),
        P(("ep", "tp")),
        P(("ep", "tp"), None, None),
        P(("ep", "tp"), None, None),
        P(),
        P(),
        P(),
        P(),
        P(),
        P("tp", None),
        P(),
        P(),
        P(),
        P("ep", None),
        P("ep", None, "tp"),
        P("ep", None, "tp"),
        P("ep", "tp", None),
    )
    out_specs = (P("ep", None), P(("ep", "tp"), None), P(("ep", "tp"), None))
    return jax.shard_map(
        on_device, mesh=mesh, in_specs=in_specs, out_specs=out_specs, check_vma=False
    )
```
